32 devices in a mesh: sp: 8 (over z, x), tp: 4 (over y, core).
Axes of the slice: x: 2, y: 2, z: 4, core: 2. Of those that a mesh axis runs over, the one named last changes fastest.
Arguments:
- stream: bfloat16 [4096, 2048], P(('sp', 'tp')), may hold values from -6 to 6
- projected: bfloat16 [4096, 2048], P('sp', 'tp'), may hold values from -6 to 6
- segments: int32 [4096], P('sp'), may hold values from 0 to 3, never falling along the last dimension, each value on 1 to 1536 neighbouring positions
- group_weight: bfloat16 [4, 512, 512], replicated, may hold values from -0.25 to 0.25
- group_scale: float32 [2048], replicated, may hold values from 0.1 to 1.9
- out_weight: bfloat16 [2048, 2048], replicated, may hold values from -0.125 to 0.125
- ffn_gain: float32 [2048], replicated, may hold values from 0.1 to 1.9
- routes: int32 [4096, 4], P(('sp', 'tp')), may hold values from 0 to 31, all different within a row; in each aligned block of 128 rows (0 to 127, 128 to 255, ...) at most 24 rows name the same one
- route_weights: float32 [4096, 4], P(('sp', 'tp')), may hold values from 0.05 to 0.5
- expert_gate: bfloat16 [32, 2048, 1024], P(('sp', 'tp')), may hold values from -0.25 to 0.25
- expert_up: bfloat16 [32, 2048, 1024], P(('sp', 'tp')), may hold values from -0.25 to 0.25
- expert_down: bfloat16 [32, 1024, 2048], P(('sp', 'tp')), may hold values from -0.1875 to 0.1875
Outputs:
- combined: bfloat16 [4096, 2048], P(('sp', 'tp'))
The draws below stay inside these ranges and needn't reach their ends.
Inputs may be any that keep to these rules, and one draw needn't show every extreme that they name: `segments`: document numbers never fall along the positions; a document has 1 to 1536 positions, and one has exactly 1536. `routes`: each row names 4 different experts. Among the 128 rows of one device (aligned blocks), no expert is named more than 24 times, and in some blocks one is named exactly 24 times.
All inputs are finite; a program needn't handle non-finite values.
Results may differ from the reference program's by a relative error of at most 0.015.
Values may be sent and summed in bfloat16 or wider, within the bound.
No kernel may reach another device: no remote copies, remote signals or barrier semaphores. Data moves between devices by JAX's collectives and lax.ppermute only.
A program may use at most 128 MiB of HBM per device.

```python
import math
import jax
import jax.numpy as jnp
import numpy as np
from jax import lax

D = 2048
GROUPS = 4
FF = 1024
TOP = 4
TOK_DEV = 128
TOKENS = 4096
GROUP_WIDTH = 512
EXPERTS = 32
CAP = 24
DOCS = 4
DOC_MOST = 1536


def levels(key, extent, shards, low, high):
    def one(dim, shards_of):
        heights = jax.random.uniform(jax.random.fold_in(jax.random.fold_in(key, 6), dim), (shards_of,), jnp.float32, low / len(shards), high / len(shards))
        return jnp.repeat(jnp.exp(heights), extent[dim] // shards_of).reshape((-1,) + (1,) * (len(extent) - dim - 1))

    loudness = one(*shards[0])
    for cut in shards[1:]:
        loudness = loudness * one(*cut)
    return loudness


def split_up(count, total, bound, skew):
    loads = [(1 << 20) // math.isqrt(standing ** skew) + 1 for standing in range(2, count + 1)]
    rest, given = total - bound - (count - 1), [1] * (count - 1)
    while rest > 0:
        candidates = [i for i in range(count - 1) if given[i] < bound]
        pool, remaining = sum([loads[i] for i in candidates]), rest
        for i in candidates:
            extra = min(bound - given[i], max(1, remaining * loads[i] // pool), rest)
            given[i] = given[i] + extra
            rest = rest - extra
    return np.array([bound] + given)


def ragged_sizes(own_key, number_of, total, most, skew):
    if number_of == 2:
        one = jax.random.randint(own_key, (), max(1, total - most), min(most, total - 1) + 1)
        return jnp.stack([one, total - one])
    lengths = jnp.asarray(split_up(number_of, total, most, skew), jnp.int32)
    couples = (number_of - 1) // 2
    source_of, taker = lengths[1:1 + 2 * couples:2], lengths[2:2 + 2 * couples:2]
    room = jnp.minimum(source_of - 1, most - taker)
    passed = jax.random.randint(jax.random.fold_in(own_key, 1), (couples,), 0, 1 << 20) % (room + 1)
    lengths = lengths.at[1:1 + 2 * couples:2].set(source_of - passed).at[2:2 + 2 * couples:2].set(taker + passed)
    return lengths[jax.random.permutation(jax.random.fold_in(own_key, 2), number_of)]


def deal_out(own_key, own, number, rows, number_of, top, most, lean):
    ranking = jax.random.permutation(own_key, number_of)
    crowded, usual = load_shares(number_of, rows * top, most, lean, True), load_shares(number_of, rows * top, most, lean, False)
    places = jnp.arange(number_of)

    def named(lengths, turn):
        used = int((lengths > 0).sum())
        fixed = max(1, used // 4)
        passed = fixed + (places - fixed + turn * (used - fixed)) % max(1, number_of - fixed)
        return jnp.zeros((number_of,), jnp.int32).at[ranking[jnp.where(places < fixed, places, passed)]].set(jnp.asarray(lengths, jnp.int32))

    lengths = jnp.where(number % 4 == 0, named(crowded, number // 4), named(usual, number - number // 4 - 1))
    mixed = jax.random.permutation(jax.random.fold_in(own, 3), number_of)
    giver, taker = mixed[0:number_of // 2 * 2:2], mixed[1:number_of // 2 * 2:2]
    margin = jnp.minimum(lengths[giver] - 1, most - lengths[taker]) // 2
    margin = jnp.where((giver == ranking[0]) | (taker == ranking[0]) | (lengths[taker] == 0), 0, jnp.maximum(margin, 0))
    passed = jax.random.randint(jax.random.fold_in(own, 4), (number_of // 2,), 0, 1 << 20) % (margin + 1)
    lengths = lengths.at[giver].add(-passed).at[taker].add(passed)
    labels = jnp.searchsorted(jnp.cumsum(lengths), jnp.arange(rows * top), side="right").astype(jnp.int32)
    table = labels.reshape(top, rows).T
    table = table[jax.random.permutation(jax.random.fold_in(own, 1), rows)]
    turn = jax.random.randint(jax.random.fold_in(own, 2), (rows, 1), 0, top)
    return jnp.take_along_axis(table, (jnp.arange(top)[None, :] + turn) % top, axis=1)


def load_shares(count, total, limit, skew, full):
    weights = [(1 << 20) // math.isqrt(rank ** skew) + 1 for rank in range(1, count + 1)]
    largest = limit if full else min(limit, max(-(-total // count), total * weights[0] // sum(weights)))
    least = 1 if total - largest >= count - 1 else 0
    holding, rest = [largest] + [least] * (count - 1), total - largest - least * (count - 1)
    while rest > 0:
        candidates = [i for i in range(1, count) if holding[i] < largest] or [i for i in range(1, count) if holding[i] < limit]
        pool, remaining = sum([weights[i] for i in candidates]), rest
        for i in candidates:
            addition = min(limit - holding[i], max(1, remaining * weights[i] // pool), rest)
            holding[i] = holding[i] + addition
            rest = rest - addition
    return np.array(holding)


def centred(stream_key, dims, spread, limit, cuts=(), kind=jnp.bfloat16):
    entries = spread * jax.random.normal(stream_key, dims, jnp.float32)
    if cuts:
        entries = entries * levels(stream_key, dims, cuts, -0.22, 0.18)
    return jnp.clip(entries, -limit, limit).astype(kind)


def setup_inputs(seed: int = 0) -> dict:
    streams_of = jax.random.split(jax.random.key(seed), 13)
    stream = centred(streams_of[0], (TOKENS, D), 1.0, 6.0, ((0, 32),))
    projected = centred(streams_of[1], (TOKENS, D), 1.0, 6.0, ((0, 8), (1, 4)))
    segments = jnp.searchsorted(jnp.cumsum(ragged_sizes(streams_of[2], DOCS, TOKENS, DOC_MOST, 2)), jnp.arange(TOKENS), side="right").astype(jnp.int32)
    group_weight = centred(streams_of[3], (GROUPS, GROUP_WIDTH, GROUP_WIDTH), GROUP_WIDTH ** -0.5, 0.25)
    group_scale = jnp.clip(1.0 + 0.18 * jax.random.normal(streams_of[4], (D,), jnp.float32), 0.1, 1.9)
    out_weight = centred(streams_of[5], (D, D), D ** -0.5, 0.125)
    ffn_gain = jnp.clip(1.0 + 0.18 * jax.random.normal(streams_of[6], (D,), jnp.float32), 0.1, 1.9)
    routes_keys = jax.random.split(jax.random.fold_in(streams_of[7], 1), TOKENS // TOK_DEV)
    routes_turns = jax.random.permutation(jax.random.fold_in(streams_of[7], 3), TOKENS // TOK_DEV)
    routes = jax.vmap(lambda own, number: deal_out(jax.random.fold_in(streams_of[7], 2), own, number, TOK_DEV, EXPERTS, TOP, CAP, 2))(routes_keys, routes_turns).reshape((TOKENS, TOP))
    route_weights = jnp.clip(0.05 + 0.45 * jax.random.uniform(streams_of[8], (TOKENS, TOP), jnp.float32) ** levels(streams_of[8], (TOKENS, TOP), ((0, 32),), -0.2, 0.2), 0.05, 0.5)
    expert_gate = centred(streams_of[9], (EXPERTS, D, FF), (D // 4) ** -0.5, 0.25, ((0, 32),))
    expert_up = centred(streams_of[10], (EXPERTS, D, FF), (D // 4) ** -0.5, 0.25, ((0, 32),))
    expert_down = centred(streams_of[11], (EXPERTS, FF, D), FF ** -0.5, 0.1875, ((0, 32),))
    return {"stream": stream, "projected": projected, "segments": segments, "group_weight": group_weight, "group_scale": group_scale, "out_weight": out_weight, "ffn_gain": ffn_gain, "routes": routes, "route_weights": route_weights, "expert_gate": expert_gate, "expert_up": expert_up, "expert_down": expert_down}


norm_eps = 1e-05
clamp_limit = 7.0
sigmoid_alpha = 1.702
longest_window = 16

def pool_residue(projected, segments):
    length, channels = projected.shape
    values = projected.astype(jnp.float32)
    channel = jnp.arange(channels, dtype=jnp.int32)
    window = jnp.left_shift(jnp.full((channels,), 2, jnp.int32), channel // (channels // GROUPS))
    window_sum = jnp.zeros((length, channels), jnp.float32)
    window_count = jnp.zeros((length, channels), jnp.float32)
    for offset in range(longest_window):
        earlier_rows = jnp.pad(values, ((offset, 0), (0, 0)))[:length]
        earlier_docs = jnp.pad(segments, (offset, 0), constant_values=-1)[:length]
        included = (earlier_docs == segments)[:, None] & (offset < window)[None, :]
        window_sum = window_sum + jnp.where(included, earlier_rows, jnp.float32(0.0))
        window_count = window_count + included.astype(jnp.float32)
    return (window_sum / window_count - values).astype(jnp.bfloat16)

def rms_scale(resid, gain):
    values = resid.astype(jnp.float32)
    inverse = lax.rsqrt(lax.optimization_barrier(jnp.mean(values * values, -1, keepdims=True)) + norm_eps)
    return (values * inverse * gain.astype(jnp.float32)).astype(jnp.bfloat16)

def run_expert(block, gate_matrix, up_matrix, down_matrix):
    leading = block.shape[:-1]
    flat_rows = block.reshape(-1, block.shape[-1])
    gate_value = jnp.dot(flat_rows, gate_matrix, preferred_element_type=jnp.float32)
    up_value = jnp.dot(flat_rows, up_matrix, preferred_element_type=jnp.float32)
    gated = jnp.minimum(gate_value, clamp_limit)
    linear = jnp.clip(up_value, -clamp_limit, clamp_limit)
    activated = (gated * jax.nn.sigmoid(sigmoid_alpha * gated) * (linear + 1.0)).astype(jnp.bfloat16)
    result = jnp.dot(activated, down_matrix, preferred_element_type=jnp.float32).astype(jnp.bfloat16)
    return result.reshape(leading + (down_matrix.shape[1],))

def reference(stream, projected, segments, group_weight, group_scale, out_weight, ffn_gain, routes, route_weights, expert_gate, expert_up, expert_down):
    mixed = pool_residue(projected, segments)
    length, model_width = mixed.shape
    group_width = model_width // GROUPS
    grouped = jnp.einsum('rgc,gcd->rgd', mixed.reshape(length, GROUPS, group_width).astype(jnp.float32), group_weight.astype(jnp.float32)).reshape(length, model_width)
    scaled = (grouped * group_scale.astype(jnp.float32)).astype(jnp.bfloat16)
    mixer_out = jnp.dot(scaled, out_weight, preferred_element_type=jnp.float32)
    resid = (stream.astype(jnp.float32) + mixer_out).astype(jnp.bfloat16)
    normed = rms_scale(resid, ffn_gain)
    flat_routes = routes.reshape(-1)
    flat_weights = route_weights.reshape(-1)
    token_of = jnp.arange(flat_routes.shape[0], dtype=jnp.int32) // TOP
    most_rows = EXPERTS * CAP

    def one_expert(carry, inputs):
        expert_id, gate_matrix, up_matrix, down_matrix = inputs
        matches = flat_routes == expert_id
        picked = jnp.nonzero(matches, size=most_rows, fill_value=0)[0].astype(jnp.int32)
        live = jnp.arange(most_rows, dtype=jnp.int32) < jnp.sum(matches.astype(jnp.int32))
        tokens_in = token_of[picked]
        expert_out = run_expert(normed[tokens_in], gate_matrix, up_matrix, down_matrix)
        weighting = jnp.where(live, flat_weights[picked], jnp.float32(0.0))
        carry = carry.at[tokens_in].add(expert_out.astype(jnp.float32) * weighting[:, None])
        return (carry, None)
    moe_sum, unused = lax.scan(one_expert, jnp.zeros((length, model_width), jnp.float32), (jnp.arange(EXPERTS, dtype=jnp.int32), expert_gate, expert_up, expert_down))
    return (resid.astype(jnp.float32) + moe_sum).astype(jnp.bfloat16)
```

```python
import functools

import jax
import jax.numpy as jnp
from jax import lax
from jax.experimental import pallas as pl
from jax.experimental.pallas import tpu as pltpu
from jax.sharding import PartitionSpec as P

GROUPS = 4

norm_eps = 1e-05
clamp_limit = 7.0
sigmoid_alpha = 1.702
longest_window = 16
VMEM_BYTES = 56 * 1024 * 1024


def dot32(a, b):
    return jnp.dot(a, b, preferred_element_type=jnp.float32)


def pool_kernel(first_ref, rim_ref, rows_ref, docs_ref, out_ref, *, group_width, span):
    row_count, channels = rows_ref.shape
    rim = rim_ref.shape[0]
    block = min(row_count, 128)
    first_group = first_ref[0] // group_width
    groups_here = max(1, channels // group_width)
    width = channels // groups_here
    wide = block + rim
    docs = docs_ref[...]
    rim_docs = (rim_ref[0:1, 0:rim].astype(jnp.float32) - 1.0).astype(jnp.int32)
    at_row = lax.broadcasted_iota(jnp.int32, (block, wide), 0)
    at_col = lax.broadcasted_iota(jnp.int32, (block, wide), 1)
    for start in range(0, row_count, block):
        here = docs[:, start : start + block]
        if start == 0:
            before, before_rows = rim_docs, rim_ref[...]
        else:
            before = docs[:, start - rim : start]
            before_rows = rows_ref[start - rim : start, :]
        col_docs = jnp.concatenate([before, here], 1)
        row_docs = jnp.sum(
            jnp.where(at_col == at_row + rim, jnp.broadcast_to(col_docs, (block, wide)), 0),
            1,
            keepdims=True,
        )
        back = at_row + rim - at_col
        alike = (col_docs == row_docs) & (back >= 0)
        own = rows_ref[start : start + block, :]
        values = jnp.concatenate([before_rows, own], 0)
        for part in range(groups_here):
            window = jnp.left_shift(2, first_group + part)
            band = jnp.where(alike & (back < window), 1.0, 0.0)
            count = jnp.sum(band, 1, keepdims=True)
            lanes = slice(part * width, (part + 1) * width)
            total = dot32(band.astype(jnp.bfloat16), values[:, lanes])
            out_ref[start : start + block, lanes] = (
                total / count - own[:, lanes].astype(jnp.float32)
            ).astype(jnp.bfloat16)


def pool(first, rim, rows, docs, group_width):
    return pl.pallas_call(
        functools.partial(pool_kernel, group_width=group_width, span=longest_window),
        out_shape=jax.ShapeDtypeStruct(rows.shape, jnp.bfloat16),
        in_specs=[
            pl.BlockSpec(memory_space=pltpu.SMEM),
            pl.BlockSpec(memory_space=pltpu.VMEM),
            pl.BlockSpec(memory_space=pltpu.VMEM),
            pl.BlockSpec(memory_space=pltpu.VMEM),
        ],
        out_specs=pl.BlockSpec(memory_space=pltpu.VMEM),
        name="pool",
    )(first, rim, rows, docs)


def slot_table(routes_t, experts, capacity):
    top, tokens = routes_t.shape
    expert = lax.broadcasted_iota(jnp.int32, (experts, tokens), 0)
    named = jnp.zeros((experts, tokens), jnp.bool_)
    for j in range(top):
        named = named | (routes_t[j : j + 1, :] == expert)
    earlier = (
        lax.broadcasted_iota(jnp.int32, (tokens, tokens), 0)
        < lax.broadcasted_iota(jnp.int32, (tokens, tokens), 1)
    )
    ones = jnp.where(named, 1.0, 0.0)
    rank = dot32(ones.astype(jnp.bfloat16), jnp.where(earlier, 1.0, 0.0).astype(jnp.bfloat16))
    held = jnp.where(named, rank, -1.0).astype(jnp.bfloat16)
    slots = experts * capacity
    low = lax.broadcasted_iota(jnp.int32, (slots, experts), 1) * capacity
    slot = lax.broadcasted_iota(jnp.int32, (slots, experts), 0)
    spread = jnp.where((slot >= low) & (slot < low + capacity), 1.0, 0.0).astype(jnp.bfloat16)
    within = slot - jnp.where((slot >= low) & (slot < low + capacity), low, 0)
    place = jnp.sum(
        jnp.where((slot >= low) & (slot < low + capacity), slot - low, 0), 1, keepdims=True
    ).astype(jnp.float32)
    del within
    return dot32(spread, held) == place, spread


def mixer_kernel(
    mixed_ref, gw_ref, gs_ref, ow_ref, stream_ref, gain_ref, routes_ref, resid_ref, send_ref,
    *, capacity, experts,
):
    groups, width, _ = gw_ref.shape
    parts = []
    for g in range(groups):
        lanes = slice(g * width, (g + 1) * width)
        grouped = dot32(mixed_ref[:, lanes], gw_ref[g])
        parts.append((grouped * gs_ref[:, lanes]).astype(jnp.bfloat16))
    scaled = jnp.concatenate(parts, 1)
    mixer_out = dot32(scaled, ow_ref[...])
    resid = (stream_ref[...].astype(jnp.float32) + mixer_out).astype(jnp.bfloat16)
    resid_ref[...] = resid
    values = resid.astype(jnp.float32)
    inverse = lax.rsqrt(jnp.mean(values * values, -1, keepdims=True) + norm_eps)
    normed = (values * inverse * gain_ref[...]).astype(jnp.bfloat16)
    taken, _ = slot_table(routes_ref[...], experts, capacity)
    pick = jnp.where(taken, 1.0, 0.0).astype(jnp.bfloat16)
    send_ref[...] = dot32(pick, normed).astype(jnp.bfloat16)


def mixer(mixed, gw, gs, ow, stream, gain, routes_t, experts, capacity):
    tokens, width = mixed.shape
    return pl.pallas_call(
        functools.partial(mixer_kernel, capacity=capacity, experts=experts),
        out_shape=(
            jax.ShapeDtypeStruct((tokens, width), jnp.bfloat16),
            jax.ShapeDtypeStruct((experts * capacity, width), jnp.bfloat16),
        ),
        in_specs=[pl.BlockSpec(memory_space=pltpu.VMEM)] * 7,
        out_specs=(pl.BlockSpec(memory_space=pltpu.VMEM),) * 2,
        compiler_params=pltpu.CompilerParams(vmem_limit_bytes=VMEM_BYTES),
        name="mixer",
    )(mixed, gw, gs.reshape(1, -1), ow, stream, gain.reshape(1, -1), routes_t)


def combine_kernel(resid_ref, back_ref, routes_ref, weights_ref, out_ref, *, capacity, experts):
    routes_t, weights_t = routes_ref[...], weights_ref[...]
    top, tokens = routes_t.shape
    taken, spread = slot_table(routes_t, experts, capacity)
    expert = lax.broadcasted_iota(jnp.int32, (experts, tokens), 0)
    weight = jnp.zeros((experts, tokens), jnp.float32)
    for j in range(top):
        weight = weight + jnp.where(routes_t[j : j + 1, :] == expert, weights_t[j : j + 1, :], 0.0)
    high = weight.astype(jnp.bfloat16)
    low = (weight - high.astype(jnp.float32)).astype(jnp.bfloat16)
    back = back_ref[...]
    total = resid_ref[...].astype(jnp.float32)
    for piece in (high, low):
        factor = jnp.where(taken, dot32(spread, piece), 0.0).astype(jnp.bfloat16)
        total = total + lax.dot_general(
            factor, back, (((0,), (0,)), ((), ())), preferred_element_type=jnp.float32
        )
    out_ref[...] = total.astype(jnp.bfloat16)


def combine(resid, back, routes_t, weights_t, experts, capacity):
    return pl.pallas_call(
        functools.partial(combine_kernel, capacity=capacity, experts=experts),
        out_shape=jax.ShapeDtypeStruct(resid.shape, jnp.bfloat16),
        in_specs=[pl.BlockSpec(memory_space=pltpu.VMEM)] * 4,
        out_specs=pl.BlockSpec(memory_space=pltpu.VMEM),
        compiler_params=pltpu.CompilerParams(vmem_limit_bytes=VMEM_BYTES),
        name="combine",
    )(resid, back, routes_t, weights_t)


def run_expert(rows, gate_matrix, up_matrix, down_matrix):
    gate_value = dot32(rows, gate_matrix)
    up_value = dot32(rows, up_matrix)
    gated = jnp.minimum(gate_value, clamp_limit)
    linear = jnp.clip(up_value, -clamp_limit, clamp_limit)
    activated = (gated * jax.nn.sigmoid(sigmoid_alpha * gated) * (linear + 1.0)).astype(
        jnp.bfloat16
    )
    return dot32(activated, down_matrix).astype(jnp.bfloat16)


def body(
    stream,
    projected,
    segments,
    group_weight,
    group_scale,
    out_weight,
    ffn_gain,
    routes,
    route_weights,
    expert_gate,
    expert_up,
    expert_down,
):
    row_count, channels = projected.shape
    tp_count = lax.axis_size("tp")
    sp_count = lax.axis_size("sp")
    model_width = channels * tp_count
    group_width = model_width // GROUPS
    rim = longest_window
    tail_docs = (segments[row_count - rim :] + 1).astype(jnp.bfloat16)
    payload = jnp.concatenate(
        [
            jnp.pad(tail_docs, (0, channels - rim))[None, :],
            projected[row_count - rim + 1 :],
        ],
        0,
    )
    before = lax.ppermute(payload, "sp", [(i, i + 1) for i in range(sp_count - 1)])
    first = (lax.axis_index("tp") * channels).reshape(1)
    mixed = pool(first, before, projected, segments[None, :], group_width)
    tokens_here = lax.all_to_all(mixed, "tp", split_axis=0, concat_axis=1, tiled=True)
    tok_count, top_count = routes.shape
    expert_count = sp_count * tp_count
    capacity = 3 * tok_count * top_count // (2 * expert_count)
    routes_t = routes.T
    resid, outgoing = mixer(
        tokens_here, group_weight, group_scale, out_weight, stream, ffn_gain, routes_t,
        expert_count, capacity,
    )
    arrived = lax.all_to_all(
        outgoing.reshape(expert_count, capacity, model_width),
        ("sp", "tp"), split_axis=0, concat_axis=0, tiled=True,
    ).reshape(expert_count * capacity, model_width)
    results = run_expert(arrived, expert_gate[0], expert_up[0], expert_down[0])
    returned = lax.all_to_all(
        results.reshape(expert_count, capacity, model_width),
        ("sp", "tp"), split_axis=0, concat_axis=0, tiled=True,
    ).reshape(expert_count * capacity, model_width)
    return combine(resid, returned, routes_t, route_weights.T, expert_count, capacity)


def solution(mesh):
    in_specs = (
        P(("sp", "tp"), None),
        P("sp", "tp"),
        P("sp"),
        P(),
        P(),
        P(),
        P(),
        P(("sp", "tp"), None),
        P(("sp", "tp"), None),
        P(("sp", "tp"), None, None),
        P(("sp", "tp"), None, None),
        P(("sp", "tp"), None, None),
    )
    out_specs = P(("sp", "tp"), None)
    return jax.shard_map(body, mesh=mesh, in_specs=in_specs, out_specs=out_specs, check_vma=False)
```

```python
import functools

import jax
import jax.numpy as jnp
from jax import lax
from jax.experimental import pallas as pl
from jax.experimental.pallas import tpu as pltpu
from jax.sharding import PartitionSpec as P


GROUPS = 4

norm_eps = 1e-05
clamp_limit = 7.0
sigmoid_alpha = 1.702
longest_window = 16
VMEM_BYTES = 12 * 1024 * 1024
EXPERT_BYTES = 30 * 1024 * 1024


def dot32(a, b):
    return jnp.dot(a, b, preferred_element_type=jnp.float32)


def pool_kernel(
    place_ref, rim_ref, rows_ref, docs_ref, *refs, group_width,
):
    out_refs, ext_ref = refs[:-1], refs[-1]
    _, channels = rows_ref.shape
    rim = rim_ref.shape[0]
    block = out_refs[0].shape[0]
    group, mine, edge = place_ref[0], place_ref[1], place_ref[2]
    groups_here = max(1, channels // group_width)
    width = channels // groups_here
    wide = block + rim
    ext_ref[0:rim, :] = rim_ref[...]
    ext_ref[rim:, :] = rows_ref[...]
    rim_docs = (rim_ref[0:1, 0:rim].astype(jnp.float32) - 1.0).astype(jnp.int32)
    rim_docs = jnp.where(edge == 0, -1, rim_docs)
    at_row = lax.broadcasted_iota(jnp.int32, (block, wide), 0)
    at_col = lax.broadcasted_iota(jnp.int32, (block, wide), 1)
    back = at_row + rim - at_col
    for d in range(len(out_refs)):
        index = mine ^ d
        here = docs_ref[pl.ds(index, 1), :]
        previous = docs_ref[pl.ds(jnp.maximum(index - 1, 0), 1), :][:, block - rim :]
        before = jnp.where(index == 0, rim_docs, previous)
        col_docs = jnp.concatenate([before, here], 1)
        row_docs = jnp.sum(
            jnp.where(back == 0, jnp.broadcast_to(col_docs, (block, wide)), 0), 1, keepdims=True
        )
        alike = (col_docs == row_docs) & (back >= 0)
        start = pl.multiple_of(index * block, block)
        values = ext_ref[pl.ds(start, wide), :]
        own = values[rim:, :].astype(jnp.float32)
        for part in range(groups_here):
            window = jnp.left_shift(2, group + part)
            band = jnp.where(alike & (back < window), 1.0, 0.0)
            count = jnp.sum(band, 1, keepdims=True)
            lanes = slice(part * width, (part + 1) * width)
            total = dot32(band.astype(jnp.bfloat16), values[:, lanes])
            out_refs[d][:, lanes] = (total / count - own[:, lanes]).astype(jnp.bfloat16)


def named_experts(routes_t, plane, count):
    experts = lax.broadcasted_iota(jnp.int32, (count, routes_t.shape[1]), 0)
    here = experts + plane * count
    return [routes_t[j : j + 1, :] == here for j in range(routes_t.shape[0])]


def slot_table(matches, capacity):
    count, tokens = matches[0].shape
    named = matches[0]
    for match in matches[1:]:
        named = named | match
    earlier = (
        lax.broadcasted_iota(jnp.int32, (tokens, tokens), 0)
        < lax.broadcasted_iota(jnp.int32, (tokens, tokens), 1)
    )
    ones = jnp.where(named, 1.0, 0.0)
    rank = dot32(ones.astype(jnp.bfloat16), jnp.where(earlier, 1.0, 0.0).astype(jnp.bfloat16))
    held = jnp.where(named, rank, -1.0).astype(jnp.bfloat16)
    slots = count * capacity
    low = lax.broadcasted_iota(jnp.int32, (slots, count), 1) * capacity
    slot = lax.broadcasted_iota(jnp.int32, (slots, count), 0)
    inside = (slot >= low) & (slot < low + capacity)
    spread = jnp.where(inside, 1.0, 0.0).astype(jnp.bfloat16)
    place = jnp.sum(jnp.where(inside, slot - low, 0), 1, keepdims=True).astype(jnp.float32)
    return dot32(spread, held) == place, spread


def pick_rows(where_ref, routes_t, rows, send_ref, capacity):
    count = send_ref.shape[0] // capacity
    taken, _ = slot_table(named_experts(routes_t, where_ref[0], count), capacity)
    send_ref[...] = dot32(jnp.where(taken, 1.0, 0.0).astype(jnp.bfloat16), rows).astype(
        jnp.bfloat16
    )


def mixer_kernel(
    where_ref, table_ref, gs_ref, stream_ref, gain_ref, *refs, capacity,
):
    block_refs = refs[:-9]
    gw_src, ow_src, resid_ref, chunk_ref, send_ref, mixed_ref, gw_ref, ow_ref, sems = refs[-9:]
    groups, width, _ = gw_ref.shape

    def piece(g):
        rows = pl.ds(g * width, width)
        return (
            pltpu.make_async_copy(gw_src.at[g], gw_ref.at[g], sems.at[0, g]),
            pltpu.make_async_copy(ow_src.at[rows, :], ow_ref.at[rows, :], sems.at[1, g]),
        )

    for k in range(2):
        for g in range(groups):
            piece(g)[k].start()
    tokens, _ = block_refs[0].shape
    for d in range(len(block_refs)):
        mixed_ref[where_ref[1] ^ d] = block_refs[d][...]
    mixed = jnp.concatenate([mixed_ref[d] for d in range(len(block_refs))], 1)
    parts = []
    for g in range(groups):
        lanes = slice(g * width, (g + 1) * width)
        piece(g)[0].wait()
        grouped = dot32(mixed[:, lanes], gw_ref[g])
        parts.append((grouped * gs_ref[:, lanes]).astype(jnp.bfloat16))
    mixer_out = jnp.zeros((tokens, stream_ref.shape[1]), jnp.float32)
    for g in range(groups):
        piece(g)[1].wait()
        mixer_out = mixer_out + dot32(parts[g], ow_ref[g * width : (g + 1) * width, :])
    resid = (stream_ref[...].astype(jnp.float32) + mixer_out).astype(jnp.bfloat16)
    resid_ref[...] = resid
    values = resid.astype(jnp.float32)
    inverse = lax.rsqrt(jnp.mean(values * values, -1, keepdims=True) + norm_eps)
    normed = (values * inverse * gain_ref[...]).astype(jnp.bfloat16)
    chunk_ref[0:tokens, :] = normed
    top = table_ref.shape[0] // 2
    weights = table_ref[top:, :]
    high = weights.astype(jnp.bfloat16)
    low = (weights - high.astype(jnp.float32)).astype(jnp.bfloat16)
    routes_t = table_ref[0:top, :]
    lines = [piece.astype(jnp.float32)[j : j + 1, :] for piece in (routes_t, high, low)
             for j in range(top)]
    line = jnp.concatenate(lines, 1)
    line = jnp.pad(line, ((0, 0), (0, chunk_ref.shape[1] - line.shape[1])))
    rest = chunk_ref.shape[0] - tokens
    chunk_ref[tokens:, :] = jnp.broadcast_to(line, (rest, line.shape[1])).astype(jnp.bfloat16)
    pick_rows(where_ref, routes_t.astype(jnp.int32), normed, send_ref, capacity)


def read_table(chunk_ref, tokens, top):
    line = chunk_ref[tokens:, :].astype(jnp.float32)
    rows = [line[0:1, j * tokens : (j + 1) * tokens] for j in range(3 * top)]
    pieces = [jnp.concatenate(rows[k * top : (k + 1) * top], 0) for k in range(3)]
    return pieces[0].astype(jnp.int32), pieces[1], pieces[2]


def call(kernel, shapes, args, flops, scratch=(), limit=VMEM_BYTES, in_hbm=0):
    specs = [pl.BlockSpec(memory_space=pltpu.SMEM)]
    specs += [pl.BlockSpec(memory_space=pltpu.VMEM)] * (len(args) - 1 - in_hbm)
    specs += [pl.BlockSpec(memory_space=pltpu.HBM)] * in_hbm
    return pl.pallas_call(
        kernel,
        out_shape=tuple(shapes),
        in_specs=specs,
        out_specs=(pl.BlockSpec(memory_space=pltpu.VMEM),) * len(shapes),
        scratch_shapes=scratch,
        compiler_params=pltpu.CompilerParams(vmem_limit_bytes=limit),
        cost_estimate=pl.CostEstimate(
            flops=flops, transcendentals=0, bytes_accessed=sum(a.nbytes for a in args)
        ),
    )(*args)


def pick_kernel(where_ref, chunk_ref, send_ref, *, tokens, top, capacity):
    routes_t, _, _ = read_table(chunk_ref, tokens, top)
    pick_rows(where_ref, routes_t, chunk_ref[0:tokens, :], send_ref, capacity)


def weighted_sum(where_ref, routes_t, weights, back, capacity):
    count = back.shape[0] // capacity
    matches = named_experts(routes_t, where_ref[0], count)
    taken, spread = slot_table(matches, capacity)
    total = jnp.zeros((routes_t.shape[1], back.shape[1]), jnp.float32)
    for piece in weights:
        weight = jnp.zeros(matches[0].shape, jnp.float32)
        for j, match in enumerate(matches):
            weight = weight + jnp.where(match, piece[j : j + 1, :], 0.0)
        factor = jnp.where(taken, dot32(spread, weight.astype(jnp.bfloat16)), 0.0)
        total = total + lax.dot_general(
            factor.astype(jnp.bfloat16), back, (((0,), (0,)), ((), ())),
            preferred_element_type=jnp.float32,
        )
    return total


def partial_kernel(where_ref, chunk_ref, back_ref, *refs, tokens, top, capacity):
    routes_t, high, low = read_table(chunk_ref, tokens, top)
    total = weighted_sum(where_ref, routes_t, (high, low), back_ref[...], capacity)
    for ref in refs[:-1]:
        total = total + ref[...].astype(jnp.float32)
    refs[-1][...] = total.astype(jnp.bfloat16)


def final_kernel(where_ref, chunk_ref, resid_ref, back_ref, *refs, tokens, top, capacity):
    routes_t, high, low = read_table(chunk_ref, tokens, top)
    total = weighted_sum(where_ref, routes_t, (high, low), back_ref[...], capacity)
    total = total + resid_ref[...].astype(jnp.float32)
    for ref in refs[:-1]:
        total = total + ref[...].astype(jnp.float32)
    refs[-1][...] = total.astype(jnp.bfloat16)


WEIGHT_CUTS = 4
in_hbm = functools.partial(pltpu.with_memory_space_constraint, memory_space=pltpu.HBM)


def expert_kernel(where_ref, *refs, inputs):
    row_refs, sources = refs[:inputs], refs[inputs : inputs + 3]
    out_refs = refs[inputs + 3 : 2 * inputs + 3]
    stores, sems = refs[2 * inputs + 3 : -1], refs[-1]
    gate_ref, up_ref, down_ref = stores

    def piece(k, b):
        size = stores[k].shape[0] // WEIGHT_CUTS
        part = pl.ds(b * size, size)
        return pltpu.make_async_copy(
            sources[k].at[0, part, :], stores[k].at[part, :], sems.at[k, b]
        )

    for b in range(WEIGHT_CUTS):
        piece(0, b).start()
        piece(1, b).start()
    for b in range(WEIGHT_CUTS):
        piece(2, b).start()
    rows = jnp.concatenate([ref[...] for ref in row_refs], 0)
    size = rows.shape[1] // WEIGHT_CUTS
    gate_value = up_value = None
    for b in range(WEIGHT_CUTS):
        lanes = slice(b * size, (b + 1) * size)
        piece(0, b).wait()
        part = dot32(rows[:, lanes], gate_ref[lanes, :])
        gate_value = part if b == 0 else gate_value + part
        piece(1, b).wait()
        part = dot32(rows[:, lanes], up_ref[lanes, :])
        up_value = part if b == 0 else up_value + part
    gated = jnp.minimum(gate_value, clamp_limit)
    linear = jnp.clip(up_value, -clamp_limit, clamp_limit)
    activated = (gated * jax.nn.sigmoid(sigmoid_alpha * gated) * (linear + 1.0)).astype(
        jnp.bfloat16
    )
    size = activated.shape[1] // WEIGHT_CUTS
    total = None
    for b in range(WEIGHT_CUTS):
        lanes = slice(b * size, (b + 1) * size)
        piece(2, b).wait()
        part = dot32(activated[:, lanes], down_ref[lanes, :])
        total = part if b == 0 else total + part
    result = total.astype(jnp.bfloat16)
    length = row_refs[0].shape[0]
    for i in range(inputs):
        out_refs[i][...] = result[i * length : (i + 1) * length]


def body(
    stream,
    projected,
    segments,
    group_weight,
    group_scale,
    out_weight,
    ffn_gain,
    routes,
    route_weights,
    expert_gate,
    expert_up,
    expert_down,
    *,
    planes,
):
    row_count, channels = projected.shape
    tp_count = lax.axis_size("tp")
    sp_count = lax.axis_size("sp")
    width = channels * tp_count
    group_width = width // GROUPS
    tokens, top = routes.shape
    devices = sp_count * tp_count
    count = devices // planes
    capacity = 3 * tokens * top // (2 * devices)
    hidden = expert_gate.shape[2]
    every = ("sp", "tp")
    sp_index, tp_index = lax.axis_index("sp"), lax.axis_index("tp")
    plane = (sp_index * tp_count + tp_index) // count
    where = jnp.stack([plane, tp_index]).astype(jnp.int32)
    place = jnp.stack([tp_index * channels // group_width, tp_index, sp_index]).astype(jnp.int32)
    sizes = dict(tokens=tokens, top=top, capacity=capacity)

    def hop(value):
        pairs = [(i, (i + count) % devices) for i in range(devices)]
        return lax.ppermute(value, every, pairs)

    planes_of = [list(range(p * count, (p + 1) * count)) for p in range(planes)]

    def in_plane(rows):
        blocks = rows.reshape(count, capacity, width)
        moved = lax.all_to_all(
            blocks, every, split_axis=0, concat_axis=0, axis_index_groups=planes_of,
            tiled=True,
        )
        return moved.reshape(count * capacity, width)

    rim = longest_window
    tail_docs = (segments[row_count - rim :] + 1).astype(jnp.bfloat16)
    payload = jnp.concatenate(
        [
            jnp.pad(tail_docs, (0, channels - rim))[None, :],
            projected[row_count - rim + 1 :],
        ],
        0,
    )
    before = lax.ppermute(payload, "sp", [(i, (i + 1) % sp_count) for i in range(sp_count)])
    mixed = call(
        functools.partial(pool_kernel, group_width=group_width),
        [jax.ShapeDtypeStruct((tokens, channels), jnp.bfloat16)] * tp_count,
        [place, before, projected, segments.reshape(tp_count, tokens)],
        2 * row_count * channels * (tokens + rim),
        [pltpu.VMEM((row_count + rim, channels), jnp.bfloat16)],
    )
    blocks = [mixed[0]]
    for d in range(1, tp_count):
        pairs = [(i, i ^ d) for i in range(tp_count)]
        blocks.append(lax.ppermute(mixed[d], "tp", pairs))
    table = jnp.concatenate([routes.T.astype(jnp.float32), route_weights.T], 0)

    shape = jax.ShapeDtypeStruct((tokens, width), jnp.bfloat16)
    slots = jax.ShapeDtypeStruct((count * capacity, width), jnp.bfloat16)
    resid, chunk, rows = call(
        functools.partial(mixer_kernel, capacity=capacity),
        [shape, jax.ShapeDtypeStruct((tokens + 8, width), jnp.bfloat16), slots],
        [
            where, table, group_scale.reshape(1, -1), stream, ffn_gain.reshape(1, -1),
            *blocks, in_hbm(group_weight), in_hbm(out_weight),
        ],
        2 * tokens * width * (width + group_width),
        [
            pltpu.VMEM((tp_count, tokens, channels), jnp.bfloat16),
            pltpu.VMEM(group_weight.shape, jnp.bfloat16),
            pltpu.VMEM(out_weight.shape, jnp.bfloat16),
            pltpu.SemaphoreType.DMA((2, GROUPS)),
        ],
        EXPERT_BYTES,
        2,
    )
    small = 2 * tokens * count * capacity * width

    def run_experts(groups):
        matrices = [in_hbm(expert_gate), in_hbm(expert_up), in_hbm(expert_down)]
        return call(
            functools.partial(expert_kernel, inputs=len(groups)),
            [slots] * len(groups),
            [where, *groups, *matrices],
            6 * len(groups) * groups[0].size * hidden,
            [
                pltpu.VMEM((width, hidden), jnp.bfloat16),
                pltpu.VMEM((width, hidden), jnp.bfloat16),
                pltpu.VMEM((hidden, width), jnp.bfloat16),
                pltpu.SemaphoreType.DMA((3, WEIGHT_CUTS)),
            ],
            EXPERT_BYTES,
            3,
        )

    chunks = [chunk]
    arrived = [in_plane(rows)]
    for s in range(1, planes):
        chunks.append(hop(chunks[-1]))
        (rows,) = call(functools.partial(pick_kernel, **sizes), [slots], [where, chunks[s]], small)
        arrived.append(in_plane(rows))
    first = min(2, planes)
    results = list(run_experts(arrived[:first]))
    for s in range(first, planes):
        results += run_experts([arrived[s]])
    carried = []
    for s in range(1, planes):
        back = in_plane(results[s])
        (part,) = call(
            functools.partial(partial_kernel, **sizes),
            [shape], [where, chunks[s], back, *carried], 2 * small,
        )
        carried = [hop(part)]
    back = in_plane(results[0])
    (out,) = call(
        functools.partial(final_kernel, **sizes),
        [shape], [where, chunk, resid, back, *carried], 2 * small,
    )
    return out


def plane_count(mesh):
    sizes = mesh.shape
    heights = {getattr(d, "coords", (0, 0, -1))[2] for d in mesh.devices.flat}
    if -1 in heights:
        return max(1, sizes["sp"] // max(1, sizes["tp"] // 2))
    return len(heights)


def solution(mesh):
    in_specs = (
        P(("sp", "tp"), None),
        P("sp", "tp"),
        P("sp"),
        P(),
        P(),
        P(),
        P(),
        P(("sp", "tp"), None),
        P(("sp", "tp"), None),
        P(("sp", "tp"), None, None),
        P(("sp", "tp"), None, None),
        P(("sp", "tp"), None, None),
    )
    out_specs = P(("sp", "tp"), None)
    planes = plane_count(mesh)

    def layer(*args):
        return body(*args, planes=planes)

    return jax.shard_map(layer, mesh=mesh, in_specs=in_specs, out_specs=out_specs, check_vma=False)
```

```python
import functools

import jax
import jax.numpy as jnp
from jax import lax
from jax.experimental import pallas as pl
from jax.experimental.pallas import tpu as pltpu
from jax.sharding import PartitionSpec as P


GROUPS = 4
CORES = 2

norm_eps = 1e-05
clamp_limit = 7.0
sigmoid_alpha = 1.702
longest_window = 16
VMEM_BYTES = 12 * 1024 * 1024


def dot32(a, b):
    return jnp.dot(a, b, preferred_element_type=jnp.float32)


def pool_kernel(
    place_ref, rim_ref, rows_ref, docs_ref, *refs, group_width,
):
    out_refs, ext_ref = refs[:-1], refs[-1]
    _, channels = rows_ref.shape
    rim = rim_ref.shape[0]
    block = out_refs[0].shape[0]
    group, mine, edge = place_ref[0], place_ref[1], place_ref[2]
    groups_here = max(1, channels // group_width)
    width = channels // groups_here
    wide = block + rim
    ext_ref[0:rim, :] = rim_ref[...]
    ext_ref[rim:, :] = rows_ref[...]
    rim_docs = (rim_ref[0:1, 0:rim].astype(jnp.float32) - 1.0).astype(jnp.int32)
    rim_docs = jnp.where(edge == 0, -1, rim_docs)
    at_row = lax.broadcasted_iota(jnp.int32, (block, wide), 0)
    at_col = lax.broadcasted_iota(jnp.int32, (block, wide), 1)
    back = at_row + rim - at_col
    for d in range(len(out_refs)):
        index = mine ^ d
        here = docs_ref[pl.ds(index, 1), :]
        previous = docs_ref[pl.ds(jnp.maximum(index - 1, 0), 1), :][:, block - rim :]
        before = jnp.where(index == 0, rim_docs, previous)
        col_docs = jnp.concatenate([before, here], 1)
        row_docs = jnp.sum(
            jnp.where(back == 0, jnp.broadcast_to(col_docs, (block, wide)), 0), 1, keepdims=True
        )
        alike = (col_docs == row_docs) & (back >= 0)
        start = pl.multiple_of(index * block, block)
        values = ext_ref[pl.ds(start, wide), :]
        own = values[rim:, :].astype(jnp.float32)
        for part in range(groups_here):
            window = jnp.left_shift(2, group + part)
            band = jnp.where(alike & (back < window), 1.0, 0.0)
            count = jnp.sum(band, 1, keepdims=True)
            lanes = slice(part * width, (part + 1) * width)
            total = dot32(band.astype(jnp.bfloat16), values[:, lanes])
            out_refs[d][:, lanes] = (total / count - own[:, lanes]).astype(jnp.bfloat16)


def named_experts(where_ref, routes_t, chips):
    offset = lax.broadcasted_iota(jnp.int32, (chips, routes_t.shape[1]), 0)
    here = (offset ^ where_ref[2]) * CORES + where_ref[3] + where_ref[0] * (chips * CORES)
    return [routes_t[j : j + 1, :] == here for j in range(routes_t.shape[0])]


def slot_table(matches, capacity):
    count, tokens = matches[0].shape
    named = matches[0]
    for match in matches[1:]:
        named = named | match
    earlier = (
        lax.broadcasted_iota(jnp.int32, (tokens, tokens), 0)
        < lax.broadcasted_iota(jnp.int32, (tokens, tokens), 1)
    )
    ones = jnp.where(named, 1.0, 0.0)
    rank = dot32(ones.astype(jnp.bfloat16), jnp.where(earlier, 1.0, 0.0).astype(jnp.bfloat16))
    held = jnp.where(named, rank, -1.0).astype(jnp.bfloat16)
    slots = count * capacity
    low = lax.broadcasted_iota(jnp.int32, (slots, count), 1) * capacity
    slot = lax.broadcasted_iota(jnp.int32, (slots, count), 0)
    inside = (slot >= low) & (slot < low + capacity)
    spread = jnp.where(inside, 1.0, 0.0).astype(jnp.bfloat16)
    place = jnp.sum(jnp.where(inside, slot - low, 0), 1, keepdims=True).astype(jnp.float32)
    return dot32(spread, held) == place, spread


def mixer_kernel(
    where_ref, table_ref, gs_ref, stream_ref, gain_ref, *refs
):
    gw_ref, ow_ref, *block_refs = refs[:-3]
    resid_ref, chunk_ref, mixed_ref = refs[-3:]
    groups, width, _ = gw_ref.shape
    tokens, _ = block_refs[0].shape
    for d in range(len(block_refs)):
        mixed_ref[where_ref[1] ^ d] = block_refs[d][...]
    mixed = jnp.concatenate([mixed_ref[d] for d in range(len(block_refs))], 1)
    parts = []
    for g in range(groups):
        lanes = slice(g * width, (g + 1) * width)
        grouped = dot32(mixed[:, lanes], gw_ref[g])
        parts.append((grouped * gs_ref[:, lanes]).astype(jnp.bfloat16))
    mixer_out = dot32(jnp.concatenate(parts, 1), ow_ref[...])
    resid = (stream_ref[...].astype(jnp.float32) + mixer_out).astype(jnp.bfloat16)
    resid_ref[...] = resid
    values = resid.astype(jnp.float32)
    inverse = lax.rsqrt(jnp.mean(values * values, -1, keepdims=True) + norm_eps)
    normed = (values * inverse * gain_ref[...]).astype(jnp.bfloat16)
    chunk_ref[0:tokens, :] = normed
    top = table_ref.shape[0] // 2
    weights = table_ref[top:, :]
    high = weights.astype(jnp.bfloat16)
    low = (weights - high.astype(jnp.float32)).astype(jnp.bfloat16)
    routes_t = table_ref[0:top, :]
    lines = [piece.astype(jnp.float32)[j : j + 1, :] for piece in (routes_t, high, low)
             for j in range(top)]
    line = jnp.concatenate(lines, 1)
    line = jnp.pad(line, ((0, 0), (0, chunk_ref.shape[1] - line.shape[1])))
    rest = chunk_ref.shape[0] - tokens
    chunk_ref[tokens:, :] = jnp.broadcast_to(line, (rest, line.shape[1])).astype(jnp.bfloat16)


def read_table(chunk_ref, tokens, top):
    line = chunk_ref[tokens:, :].astype(jnp.float32)
    rows = [line[0:1, j * tokens : (j + 1) * tokens] for j in range(3 * top)]
    pieces = [jnp.concatenate(rows[k * top : (k + 1) * top], 0) for k in range(3)]
    return pieces[0].astype(jnp.int32), pieces[1], pieces[2]


def call(kernel, shapes, args, flops, scratch=(), limit=VMEM_BYTES):
    specs = [pl.BlockSpec(memory_space=pltpu.SMEM)]
    specs += [pl.BlockSpec(memory_space=pltpu.VMEM)] * (len(args) - 1)
    return pl.pallas_call(
        kernel,
        out_shape=tuple(shapes),
        in_specs=specs,
        out_specs=(pl.BlockSpec(memory_space=pltpu.VMEM),) * len(shapes),
        scratch_shapes=scratch,
        compiler_params=pltpu.CompilerParams(vmem_limit_bytes=limit),
        cost_estimate=pl.CostEstimate(
            flops=flops, transcendentals=0, bytes_accessed=sum(a.nbytes for a in args)
        ),
    )(*args)


def pick_kernel(where_ref, *refs, tokens, top, capacity):
    chunk_refs, send_refs = refs[:CORES], refs[CORES:]
    chips = len(send_refs)
    for k in range(CORES):
        routes_t, _, _ = read_table(chunk_refs[k], tokens, top)
        taken, _ = slot_table(named_experts(where_ref, routes_t, chips), capacity)
        picked = dot32(jnp.where(taken, 1.0, 0.0).astype(jnp.bfloat16), chunk_refs[k][0:tokens, :])
        picked = picked.astype(jnp.bfloat16)
        for d in range(chips):
            rows = picked[d * capacity : (d + 1) * capacity]
            send_refs[d][k * capacity : (k + 1) * capacity, :] = rows


def weighted_sum(where_ref, chunk_ref, back_refs, k, tokens, top, capacity):
    routes_t, *weights = read_table(chunk_ref, tokens, top)
    matches = named_experts(where_ref, routes_t, len(back_refs))
    taken, spread = slot_table(matches, capacity)
    back = jnp.concatenate([ref[k * capacity : (k + 1) * capacity, :] for ref in back_refs], 0)
    total = jnp.zeros((tokens, back.shape[1]), jnp.float32)
    for piece in weights:
        weight = jnp.zeros(matches[0].shape, jnp.float32)
        for j, match in enumerate(matches):
            weight = weight + jnp.where(match, piece[j : j + 1, :], 0.0)
        factor = jnp.where(taken, dot32(spread, weight.astype(jnp.bfloat16)), 0.0)
        total = total + lax.dot_general(
            factor.astype(jnp.bfloat16), back, (((0,), (0,)), ((), ())),
            preferred_element_type=jnp.float32,
        )
    return total


def partner_kernel(where_ref, chunk_ref, *refs, tokens, top, capacity):
    total = weighted_sum(where_ref, chunk_ref, refs[:-1], 1, tokens, top, capacity)
    refs[-1][...] = total.astype(jnp.bfloat16)


def own_kernel(where_ref, chunk_ref, *refs, chips, tokens, top, capacity):
    total = weighted_sum(where_ref, chunk_ref, refs[:chips], 0, tokens, top, capacity)
    for ref in refs[chips:-1]:
        total = total + ref[...].astype(jnp.float32)
    refs[-1][...] = total.astype(jnp.bfloat16)


def expert_kernel(where_ref, *refs):
    chips = (len(refs) - 3) // 2
    row_refs, (gate_ref, up_ref, down_ref), out_refs = refs[:chips], refs[chips : chips + 3], refs[chips + 3 :]
    rows = jnp.concatenate([ref[...] for ref in row_refs], 0)
    hidden = gate_ref.shape[1]
    cut = min(hidden, 256)
    total = None
    for start in range(0, hidden, cut):
        lanes = slice(start, start + cut)
        gated = jnp.minimum(dot32(rows, gate_ref[:, lanes]), clamp_limit)
        linear = jnp.clip(dot32(rows, up_ref[:, lanes]), -clamp_limit, clamp_limit)
        activated = (gated * jax.nn.sigmoid(sigmoid_alpha * gated) * (linear + 1.0)).astype(
            jnp.bfloat16
        )
        part = dot32(activated, down_ref[lanes, :])
        total = part if total is None else total + part
    result = total.astype(jnp.bfloat16)
    length = row_refs[0].shape[0]
    for d in range(chips):
        out_refs[d][...] = result[d * length : (d + 1) * length]


in_vmem = functools.partial(pltpu.with_memory_space_constraint, memory_space=pltpu.VMEM)


def body(
    stream,
    projected,
    segments,
    group_weight,
    group_scale,
    out_weight,
    ffn_gain,
    routes,
    route_weights,
    expert_gate,
    expert_up,
    expert_down,
    *,
    planes,
):
    row_count, channels = projected.shape
    tp_count = lax.axis_size("tp")
    sp_count = lax.axis_size("sp")
    width = channels * tp_count
    group_width = width // GROUPS
    tokens, top = routes.shape
    devices = sp_count * tp_count
    count = devices // planes
    chips = count // CORES
    capacity = 3 * tokens * top // (2 * devices)
    hidden = expert_gate.shape[2]
    every = ("sp", "tp")
    sp_index, tp_index = lax.axis_index("sp"), lax.axis_index("tp")
    device = sp_index * tp_count + tp_index
    where = jnp.stack(
        [device // count, tp_index, device % count // CORES, device % CORES]
    ).astype(jnp.int32)
    place = jnp.stack([tp_index * channels // group_width, tp_index, sp_index]).astype(jnp.int32)
    sizes = dict(tokens=tokens, top=top, capacity=capacity)

    def move(value, to):
        return lax.ppermute(value, every, [(i, to(i)) for i in range(devices)])

    def hop(value):
        return move(value, lambda i: (i + count) % devices)

    def swap(value):
        return move(value, lambda i: i ^ 1)

    def in_plane(blocks):
        moved = [blocks[0]]
        for d in range(1, chips):
            moved.append(move(blocks[d], lambda i: i ^ (d * CORES)))
        return moved

    rim = longest_window
    tail_docs = (segments[row_count - rim :] + 1).astype(jnp.bfloat16)
    payload = jnp.concatenate(
        [
            jnp.pad(tail_docs, (0, channels - rim))[None, :],
            projected[row_count - rim + 1 :],
        ],
        0,
    )
    before = lax.ppermute(payload, "sp", [(i, (i + 1) % sp_count) for i in range(sp_count)])
    mixed = call(
        functools.partial(pool_kernel, group_width=group_width),
        [jax.ShapeDtypeStruct((tokens, channels), jnp.bfloat16)] * tp_count,
        [place, before, in_vmem(projected), segments.reshape(tp_count, tokens)],
        2 * row_count * channels * (tokens + rim),
        [pltpu.VMEM((row_count + rim, channels), jnp.bfloat16)],
    )
    blocks = [mixed[0]]
    for d in range(1, tp_count):
        pairs = [(i, i ^ d) for i in range(tp_count)]
        blocks.append(lax.ppermute(mixed[d], "tp", pairs))
    table = jnp.concatenate([routes.T.astype(jnp.float32), route_weights.T], 0)

    shape = jax.ShapeDtypeStruct((tokens, width), jnp.bfloat16)
    block = jax.ShapeDtypeStruct((CORES * capacity, width), jnp.bfloat16)
    resid, chunk = call(
        mixer_kernel,
        [shape, jax.ShapeDtypeStruct((tokens + 8, width), jnp.bfloat16)],
        [
            where, table, in_vmem(group_scale.reshape(1, -1)), in_vmem(stream),
            in_vmem(ffn_gain.reshape(1, -1)), in_vmem(group_weight), in_vmem(out_weight), *blocks,
        ],
        2 * tokens * width * (width + group_width),
        [pltpu.VMEM((tp_count, tokens, channels), jnp.bfloat16)],
    )
    small = 2 * tokens * count * capacity * width
    matrices = [in_vmem(expert_gate[0]), in_vmem(expert_up[0]), in_vmem(expert_down[0])]

    def dispatch(pair):
        rows = call(
            functools.partial(pick_kernel, **sizes), [block] * chips, [where, *pair],
            small,
        )
        return in_plane(rows)

    def experts(rows):
        results = call(
            expert_kernel, [block] * chips, [where, *rows, *matrices],
            6 * count * capacity * width * hidden,
        )
        return in_plane(results)

    def gather(pair, back, others):
        (given,) = call(
            functools.partial(partner_kernel, **sizes), [shape], [where, pair[1], *back],
            small,
        )
        got = swap(given)
        (total,) = call(
            functools.partial(own_kernel, chips=chips, **sizes), [shape],
            [where, pair[0], *back, got, *others], small,
        )
        return total

    chunks = [chunk]
    for _ in range(1, planes):
        chunks.append(hop(chunks[-1]))
    pairs = [(chunks[s], swap(chunks[s])) for s in range(planes)]
    arrived = [dispatch(pairs[s]) for s in range(planes)]
    returned = [experts(arrived[s]) for s in range(planes)]
    carried = []
    for s in range(1, planes):
        carried = [hop(gather(pairs[s], returned[s], carried))]
    return gather(pairs[0], returned[0], [resid, *carried])


def plane_count(mesh):
    sizes = mesh.shape
    heights = {getattr(d, "coords", (0, 0, -1))[2] for d in mesh.devices.flat}
    if -1 in heights:
        return max(1, sizes["sp"] // max(1, sizes["tp"] // 2))
    return len(heights)


def solution(mesh):
    in_specs = (
        P(("sp", "tp"), None),
        P("sp", "tp"),
        P("sp"),
        P(),
        P(),
        P(),
        P(),
        P(("sp", "tp"), None),
        P(("sp", "tp"), None),
        P(("sp", "tp"), None, None),
        P(("sp", "tp"), None, None),
        P(("sp", "tp"), None, None),
    )
    out_specs = P(("sp", "tp"), None)
    planes = plane_count(mesh)

    def layer(*args):
        return body(*args, planes=planes)

    return jax.shard_map(layer, mesh=mesh, in_specs=in_specs, out_specs=out_specs, check_vma=False)
```

```python
import functools

import jax
import jax.numpy as jnp
from jax import lax
from jax.experimental import pallas as pl
from jax.experimental.pallas import tpu as pltpu
from jax.sharding import PartitionSpec as P


GROUPS = 4
CORES = 2
COVER_FLOPS = 40_000_000_000

norm_eps = 1e-05
clamp_limit = 7.0
sigmoid_alpha = 1.702
longest_window = 16
VMEM_BYTES = 12 * 1024 * 1024


def dot32(a, b):
    return jnp.dot(a, b, preferred_element_type=jnp.float32)


def cut_kernel(where_ref, rows_ref, docs_ref, *refs):
    out_refs, rim_ref, ext_ref = refs[:-2], refs[-2], refs[-1]
    row_count, channels = rows_ref.shape
    rim = rim_ref.shape[0]
    block = row_count // len(out_refs)
    ext_ref[0:rim, :] = jnp.zeros((rim, channels), jnp.bfloat16)
    ext_ref[rim:, :] = rows_ref[...]
    for d in range(len(out_refs)):
        start = pl.multiple_of((where_ref[1] ^ d) * block, block)
        out_refs[d][...] = ext_ref[pl.ds(start, block + rim), :]
    docs = docs_ref[docs_ref.shape[0] - 1 :, :][:, block - rim :] + 1
    line = jnp.concatenate(
        [docs.astype(jnp.float32), jnp.zeros((1, channels - rim), jnp.float32)], 1
    )
    tail = rows_ref[row_count - rim :, :].astype(jnp.float32)
    first = lax.broadcasted_iota(jnp.int32, (rim, channels), 0) == 0
    rim_ref[...] = jnp.where(first, line, tail).astype(jnp.bfloat16)


def pool_rows(where_ref, docs_ref, block_refs, rim_refs, ext_ref, groups):
    mine = where_ref[1]
    parts, tokens_rim, channels = ext_ref.shape
    rim = rim_refs[0].shape[0]
    block = tokens_rim - rim
    for d in range(parts):
        ext_ref[mine ^ d] = block_refs[d][...]

    @pl.when(mine == 0)
    def _():
        for d in range(parts):
            ext_ref[d, 0:rim, :] = rim_refs[d][...]

    rim_docs = (rim_refs[0][0:1, 0:rim].astype(jnp.float32) - 1.0).astype(jnp.int32)
    rim_docs = jnp.where(where_ref[4] == 0, -1, rim_docs)
    here = docs_ref[pl.ds(mine, 1), :]
    previous = docs_ref[pl.ds(jnp.maximum(mine - 1, 0), 1), :][:, block - rim :]
    col_docs = jnp.concatenate([jnp.where(mine == 0, rim_docs, previous), here], 1)
    at_row = lax.broadcasted_iota(jnp.int32, (block, tokens_rim), 0)
    at_col = lax.broadcasted_iota(jnp.int32, (block, tokens_rim), 1)
    back = at_row + rim - at_col
    row_docs = jnp.sum(
        jnp.where(back == 0, jnp.broadcast_to(col_docs, back.shape), 0), 1, keepdims=True
    )
    alike = (col_docs == row_docs) & (back >= 0)
    values = jnp.concatenate([ext_ref[d] for d in range(parts)], 1)
    width = parts * channels // groups
    mixed = []
    for g in range(groups):
        lanes = values[:, g * width : (g + 1) * width]
        band = jnp.where(alike & (back < 2 << g), 1.0, 0.0)
        count = jnp.sum(band, 1, keepdims=True)
        total = dot32(band.astype(jnp.bfloat16), lanes)
        mixed.append((total / count - lanes[rim:, :].astype(jnp.float32)).astype(jnp.bfloat16))
    return mixed


def named_experts(where_ref, routes_t, chips):
    offset = lax.broadcasted_iota(jnp.int32, (chips, routes_t.shape[1]), 0)
    here = (offset ^ where_ref[2]) * CORES + where_ref[3] + where_ref[0] * (chips * CORES)
    return [routes_t[j : j + 1, :] == here for j in range(routes_t.shape[0])]


def slot_table(matches, capacity):
    count, tokens = matches[0].shape
    named = matches[0]
    for match in matches[1:]:
        named = named | match
    earlier = (
        lax.broadcasted_iota(jnp.int32, (tokens, tokens), 0)
        < lax.broadcasted_iota(jnp.int32, (tokens, tokens), 1)
    )
    ones = jnp.where(named, 1.0, 0.0)
    rank = dot32(ones.astype(jnp.bfloat16), jnp.where(earlier, 1.0, 0.0).astype(jnp.bfloat16))
    held = jnp.where(named, rank, -1.0).astype(jnp.bfloat16)
    slots = count * capacity
    low = lax.broadcasted_iota(jnp.int32, (slots, count), 1) * capacity
    slot = lax.broadcasted_iota(jnp.int32, (slots, count), 0)
    inside = (slot >= low) & (slot < low + capacity)
    spread = jnp.where(inside, 1.0, 0.0).astype(jnp.bfloat16)
    place = jnp.sum(jnp.where(inside, slot - low, 0), 1, keepdims=True).astype(jnp.float32)
    return dot32(spread, held) == place, spread


def mixer_kernel(
    where_ref, routes_ref, weights_ref, docs_ref, gs_ref, stream_ref, gain_ref, gw_ref, ow_ref,
    *refs
):
    resid_ref, upper_ref, lower_ref, ext_ref = refs[-4:]
    parts = ext_ref.shape[0]
    groups, width, _ = gw_ref.shape
    tokens = stream_ref.shape[0]
    mixed = pool_rows(where_ref, docs_ref, refs[:parts], refs[parts : 2 * parts], ext_ref, groups)
    scaled = []
    for g in range(groups):
        lanes = slice(g * width, (g + 1) * width)
        scaled.append((dot32(mixed[g], gw_ref[g]) * gs_ref[:, lanes]).astype(jnp.bfloat16))
    mixer_out = dot32(jnp.concatenate(scaled, 1), ow_ref[...])
    resid = (stream_ref[...].astype(jnp.float32) + mixer_out).astype(jnp.bfloat16)
    resid_ref[...] = resid
    values = resid.astype(jnp.float32)
    inverse = lax.rsqrt(jnp.mean(values * values, -1, keepdims=True) + norm_eps)
    normed = (values * inverse * gain_ref[...]).astype(jnp.bfloat16)
    half = upper_ref.shape[0]
    upper_ref[...] = normed[0:half]
    lower_ref[0 : tokens - half, :] = normed[half:]
    top = routes_ref.shape[0]
    weights = weights_ref[...]
    high = weights.astype(jnp.bfloat16)
    low = (weights - high.astype(jnp.float32)).astype(jnp.bfloat16)
    routes_t = routes_ref[...]
    lines = [piece.astype(jnp.float32)[j : j + 1, :] for piece in (routes_t, high, low)
             for j in range(top)]
    line = jnp.concatenate(lines, 1)
    line = jnp.pad(line, ((0, 0), (0, lower_ref.shape[1] - line.shape[1])))
    rest = lower_ref.shape[0] - (tokens - half)
    lower_ref[tokens - half :, :] = jnp.broadcast_to(line, (rest, line.shape[1])).astype(jnp.bfloat16)


def read_table(lower_ref, tokens, top):
    line = lower_ref[lower_ref.shape[0] - 8 :, :].astype(jnp.float32)
    rows = [line[0:1, j * tokens : (j + 1) * tokens] for j in range(3 * top)]
    pieces = [jnp.concatenate(rows[k * top : (k + 1) * top], 0) for k in range(3)]
    return pieces[0].astype(jnp.int32), pieces[1], pieces[2]


def call(kernel, shapes, args, flops, scratch=(), limit=VMEM_BYTES):
    specs = [pl.BlockSpec(memory_space=pltpu.SMEM)]
    specs += [pl.BlockSpec(memory_space=pltpu.VMEM)] * (len(args) - 1)
    return pl.pallas_call(
        kernel,
        out_shape=tuple(shapes),
        in_specs=specs,
        out_specs=(pl.BlockSpec(memory_space=pltpu.VMEM),) * len(shapes),
        scratch_shapes=scratch,
        compiler_params=pltpu.CompilerParams(vmem_limit_bytes=limit),
        cost_estimate=pl.CostEstimate(
            flops=flops, transcendentals=0, bytes_accessed=sum(a.nbytes for a in args)
        ),
    )(*args)


def pick_kernel(where_ref, *refs, tokens, top, capacity):
    chunk_refs, send_refs = refs[: 2 * CORES], refs[2 * CORES :]
    chips = len(send_refs)
    for k in range(CORES):
        upper_ref, lower_ref = chunk_refs[2 * k : 2 * k + 2]
        routes_t, _, _ = read_table(lower_ref, tokens, top)
        taken, _ = slot_table(named_experts(where_ref, routes_t, chips), capacity)
        rest = tokens - upper_ref.shape[0]
        rows = jnp.concatenate([upper_ref[...], lower_ref[0:rest, :]], 0)
        picked = dot32(jnp.where(taken, 1.0, 0.0).astype(jnp.bfloat16), rows)
        picked = picked.astype(jnp.bfloat16)
        for d in range(chips):
            rows = picked[d * capacity : (d + 1) * capacity]
            send_refs[d][k * capacity : (k + 1) * capacity, :] = rows


def weighted_sum(where_ref, lower_ref, back_refs, k, tokens, top, capacity):
    routes_t, *weights = read_table(lower_ref, tokens, top)
    matches = named_experts(where_ref, routes_t, len(back_refs))
    taken, spread = slot_table(matches, capacity)
    back = jnp.concatenate([ref[k * capacity : (k + 1) * capacity, :] for ref in back_refs], 0)
    total = jnp.zeros((tokens, back.shape[1]), jnp.float32)
    for piece in weights:
        weight = jnp.zeros(matches[0].shape, jnp.float32)
        for j, match in enumerate(matches):
            weight = weight + jnp.where(match, piece[j : j + 1, :], 0.0)
        factor = jnp.where(taken, dot32(spread, weight.astype(jnp.bfloat16)), 0.0)
        total = total + lax.dot_general(
            factor.astype(jnp.bfloat16), back, (((0,), (0,)), ((), ())),
            preferred_element_type=jnp.float32,
        )
    return total


def share_kernel(where_ref, own_ref, other_ref, *refs, tokens, top, capacity):
    back_refs, (given_ref, kept_ref) = refs[:-2], refs[-2:]
    total = weighted_sum(where_ref, other_ref, back_refs, 1, tokens, top, capacity)
    given_ref[...] = total.astype(jnp.bfloat16)
    kept_ref[...] = weighted_sum(where_ref, own_ref, back_refs, 0, tokens, top, capacity)


def sum_kernel(where_ref, kept_ref, got_ref, *refs, start):
    size = refs[-1].shape[0]
    rows = slice(start, start + size)
    total = kept_ref[rows, :] + got_ref[rows, :].astype(jnp.float32)
    for ref in refs[:-1]:
        total = total + ref[...].astype(jnp.float32)
    refs[-1][...] = total.astype(jnp.bfloat16)


def final_kernel(where_ref, kept_ref, got_ref, resid_ref, *refs):
    total = kept_ref[...] + got_ref[...].astype(jnp.float32) + resid_ref[...].astype(jnp.float32)
    if len(refs) > 1:
        total = total + jnp.concatenate([ref[...] for ref in refs[:-1]], 0).astype(jnp.float32)
    refs[-1][...] = total.astype(jnp.bfloat16)


def expert_kernel(where_ref, *refs):
    chips = (len(refs) - 3) // 2
    row_refs, (gate_ref, up_ref, down_ref), out_refs = refs[:chips], refs[chips : chips + 3], refs[chips + 3 :]
    rows = jnp.concatenate([ref[...] for ref in row_refs], 0)
    hidden = gate_ref.shape[1]
    cut = min(hidden, 256)
    total = None
    for start in range(0, hidden, cut):
        lanes = slice(start, start + cut)
        gated = jnp.minimum(dot32(rows, gate_ref[:, lanes]), clamp_limit)
        linear = jnp.clip(dot32(rows, up_ref[:, lanes]), -clamp_limit, clamp_limit)
        activated = (gated * jax.nn.sigmoid(sigmoid_alpha * gated) * (linear + 1.0)).astype(
            jnp.bfloat16
        )
        part = dot32(activated, down_ref[lanes, :])
        total = part if total is None else total + part
    result = total.astype(jnp.bfloat16)
    length = row_refs[0].shape[0]
    for d in range(chips):
        out_refs[d][...] = result[d * length : (d + 1) * length]


in_vmem = functools.partial(pltpu.with_memory_space_constraint, memory_space=pltpu.VMEM)


def body(
    stream,
    projected,
    segments,
    group_weight,
    group_scale,
    out_weight,
    ffn_gain,
    routes,
    route_weights,
    expert_gate,
    expert_up,
    expert_down,
    *,
    planes,
):
    row_count, channels = projected.shape
    tp_count = lax.axis_size("tp")
    sp_count = lax.axis_size("sp")
    width = channels * tp_count
    group_width = width // GROUPS
    tokens, top = routes.shape
    devices = sp_count * tp_count
    count = devices // planes
    chips = count // CORES
    capacity = 3 * tokens * top // (2 * devices)
    hidden = expert_gate.shape[2]
    every = ("sp", "tp")
    sp_index, tp_index = lax.axis_index("sp"), lax.axis_index("tp")
    device = sp_index * tp_count + tp_index
    where = jnp.stack(
        [device // count, tp_index, device % count // CORES, device % CORES, sp_index]
    ).astype(jnp.int32)
    sizes = dict(tokens=tokens, top=top, capacity=capacity)

    def move(value, to):
        return lax.ppermute(value, every, [(i, to(i)) for i in range(devices)])

    def hop(value):
        return move(value, lambda i: (i + count) % devices)

    def swap(value):
        return move(value, lambda i: i ^ 1)

    def in_plane(blocks):
        moved = [blocks[0]]
        for d in range(1, chips):
            moved.append(move(blocks[d], lambda i: i ^ (d * CORES)))
        return moved

    rim = longest_window
    docs = segments.reshape(tp_count, tokens)
    part = jax.ShapeDtypeStruct((tokens + rim, channels), jnp.bfloat16)
    *cuts, tail = call(
        cut_kernel,
        [part] * tp_count + [jax.ShapeDtypeStruct((rim, channels), jnp.bfloat16)],
        [where, projected, docs],
        COVER_FLOPS,
        [pltpu.VMEM((row_count + rim, channels), jnp.bfloat16)],
    )

    def beside(i, d, ahead):
        sp, tp = i // tp_count, i % tp_count
        return (sp + ahead) % sp_count * tp_count + (tp ^ d)

    blocks, rims = [cuts[0]], []
    for d in range(1, tp_count):
        blocks.append(move(cuts[d], lambda i: beside(i, d, 0)))
    for d in range(tp_count):
        rims.append(move(tail, lambda i: beside(i, d, 1)))

    shape = jax.ShapeDtypeStruct((tokens, width), jnp.bfloat16)
    block = jax.ShapeDtypeStruct((CORES * capacity, width), jnp.bfloat16)
    half = tokens // 2
    piece = jax.ShapeDtypeStruct((half, width), jnp.bfloat16)
    resid, *chunk = call(
        mixer_kernel,
        [shape, piece, jax.ShapeDtypeStruct((tokens - half + 8, width), jnp.bfloat16)],
        [
            where, routes.T, route_weights.T, docs, in_vmem(group_scale.reshape(1, -1)),
            in_vmem(stream), in_vmem(ffn_gain.reshape(1, -1)), in_vmem(group_weight),
            in_vmem(out_weight), *blocks, *rims,
        ],
        2 * tokens * width * (width + group_width),
        [pltpu.VMEM((tp_count, tokens + rim, channels), jnp.bfloat16)],
    )
    small = 2 * tokens * count * capacity * width
    matrices = [in_vmem(expert_gate[0]), in_vmem(expert_up[0]), in_vmem(expert_down[0])]

    def dispatch(pair):
        rows = call(
            functools.partial(pick_kernel, **sizes), [block] * chips, [where, *pair],
            small,
        )
        return in_plane(rows)

    def experts(rows):
        results = call(
            expert_kernel, [block] * chips, [where, *rows, *matrices],
            6 * count * capacity * width * hidden,
        )
        return in_plane(results)

    def share(pair, back):
        given, kept = call(
            functools.partial(share_kernel, **sizes),
            [shape, jax.ShapeDtypeStruct(shape.shape, jnp.float32)],
            [where, pair[1], pair[3], *back], 2 * small,
        )
        return kept, swap(given)

    chunks = [chunk]
    for _ in range(1, planes):
        chunks.append([hop(chunks[-1][h]) for h in range(2)])
    pairs = []
    for s in range(planes):
        pairs.append(chunks[s] + [swap(chunks[s][h]) for h in range(2)])
    arrived = [dispatch(pairs[s]) for s in range(planes)]
    returned = [experts(arrived[s]) for s in range(planes)]
    carried = [[], []]
    for s in range(1, planes):
        shares = share(pairs[s], returned[s])
        for h in range(2):
            (total,) = call(
                functools.partial(sum_kernel, start=h * half), [piece],
                [where, *shares, *carried[h]], tokens * width,
            )
            carried[h] = [hop(total)]
    shares = share(pairs[0], returned[0])
    (out,) = call(
        final_kernel, [shape], [where, *shares, resid, *carried[0], *carried[1]],
        tokens * width,
    )
    return out


def plane_count(mesh):
    sizes = mesh.shape
    heights = {getattr(d, "coords", (0, 0, -1))[2] for d in mesh.devices.flat}
    if -1 in heights:
        return max(1, sizes["sp"] // max(1, sizes["tp"] // 2))
    return len(heights)


def solution(mesh):
    in_specs = (
        P(("sp", "tp"), None),
        P("sp", "tp"),
        P("sp"),
        P(),
        P(),
        P(),
        P(),
        P(("sp", "tp"), None),
        P(("sp", "tp"), None),
        P(("sp", "tp"), None, None),
        P(("sp", "tp"), None, None),
        P(("sp", "tp"), None, None),
    )
    out_specs = P(("sp", "tp"), None)
    planes = plane_count(mesh)

    def layer(*args):
        return body(*args, planes=planes)

    return jax.shard_map(layer, mesh=mesh, in_specs=in_specs, out_specs=out_specs, check_vma=False)
```

```python
import functools

import jax
import jax.numpy as jnp
from jax import lax
from jax.experimental import pallas as pl
from jax.experimental.pallas import tpu as pltpu
from jax.sharding import PartitionSpec as P


GROUPS = 4
CORES = 2
COVER_FLOPS = 40_000_000_000

norm_eps = 1e-05
clamp_limit = 7.0
sigmoid_alpha = 1.702
longest_window = 16
VMEM_BYTES = 12 * 1024 * 1024


def dot32(a, b):
    return jnp.dot(a, b, preferred_element_type=jnp.float32)


def cut_kernel(where_ref, rows_ref, docs_ref, *refs):
    out_refs, rim_ref, ext_ref = refs[:-2], refs[-2], refs[-1]
    row_count, channels = rows_ref.shape
    rim = rim_ref.shape[0]
    block = row_count // len(out_refs)
    ext_ref[0:rim, :] = jnp.zeros((rim, channels), jnp.bfloat16)
    ext_ref[rim:, :] = rows_ref[...]
    for d in range(len(out_refs)):
        start = pl.multiple_of((where_ref[1] ^ d) * block, block)
        out_refs[d][...] = ext_ref[pl.ds(start, block + rim), :]
    docs = docs_ref[docs_ref.shape[0] - 1 :, :][:, block - rim :] + 1
    line = jnp.concatenate(
        [docs.astype(jnp.float32), jnp.zeros((1, channels - rim), jnp.float32)], 1
    )
    tail = rows_ref[row_count - rim :, :].astype(jnp.float32)
    first = lax.broadcasted_iota(jnp.int32, (rim, channels), 0) == 0
    rim_ref[...] = jnp.where(first, line, tail).astype(jnp.bfloat16)


def pool_rows(where_ref, docs_ref, block_refs, rim_refs, ext_ref, groups):
    mine = where_ref[1]
    parts, tokens_rim, channels = ext_ref.shape
    rim = rim_refs[0].shape[0]
    block = tokens_rim - rim
    for d in range(parts):
        ext_ref[mine ^ d] = block_refs[d][...]

    @pl.when(mine == 0)
    def _():
        for d in range(parts):
            ext_ref[d, 0:rim, :] = rim_refs[d][...]

    rim_docs = (rim_refs[0][0:1, 0:rim].astype(jnp.float32) - 1.0).astype(jnp.int32)
    rim_docs = jnp.where(where_ref[4] == 0, -1, rim_docs)
    here = docs_ref[pl.ds(mine, 1), :]
    previous = docs_ref[pl.ds(jnp.maximum(mine - 1, 0), 1), :][:, block - rim :]
    col_docs = jnp.concatenate([jnp.where(mine == 0, rim_docs, previous), here], 1)
    at_row = lax.broadcasted_iota(jnp.int32, (block, tokens_rim), 0)
    at_col = lax.broadcasted_iota(jnp.int32, (block, tokens_rim), 1)
    back = at_row + rim - at_col
    row_docs = jnp.sum(
        jnp.where(back == 0, jnp.broadcast_to(col_docs, back.shape), 0), 1, keepdims=True
    )
    alike = (col_docs == row_docs) & (back >= 0)
    values = jnp.concatenate([ext_ref[d] for d in range(parts)], 1)
    width = parts * channels // groups
    mixed = []
    for g in range(groups):
        lanes = values[:, g * width : (g + 1) * width]
        band = jnp.where(alike & (back < 2 << g), 1.0, 0.0)
        count = jnp.sum(band, 1, keepdims=True)
        total = dot32(band.astype(jnp.bfloat16), lanes)
        mixed.append((total / count - lanes[rim:, :].astype(jnp.float32)).astype(jnp.bfloat16))
    return mixed


def slot_tables(where_ref, tables, chips, capacity):
    tokens = tables[0][0].shape[1]
    offset = lax.broadcasted_iota(jnp.int32, (chips, tokens), 0)
    here = (offset ^ where_ref[2]) * CORES + where_ref[3] + where_ref[0] * (chips * CORES)
    named, highs, lows = [], [], []
    for routes_t, high, low in tables:
        matches = [routes_t[j : j + 1, :] == here for j in range(routes_t.shape[0])]
        named.append(sum(jnp.where(m, 1.0, 0.0) for m in matches))
        highs.append(sum(jnp.where(m, high[j : j + 1, :], 0.0) for j, m in enumerate(matches)))
        lows.append(sum(jnp.where(m, low[j : j + 1, :], 0.0) for j, m in enumerate(matches)))
    named, high, low = (jnp.concatenate(parts, 0) for parts in (named, highs, lows))
    lines = named.shape[0]
    earlier = (
        lax.broadcasted_iota(jnp.int32, (tokens, tokens), 0)
        < lax.broadcasted_iota(jnp.int32, (tokens, tokens), 1)
    )
    rank = dot32(named.astype(jnp.bfloat16), jnp.where(earlier, 1.0, 0.0).astype(jnp.bfloat16))
    held = jnp.where(named > 0.0, rank, -1.0)
    slots = lines * capacity
    low_slot = lax.broadcasted_iota(jnp.int32, (slots, lines), 1) * capacity
    slot = lax.broadcasted_iota(jnp.int32, (slots, lines), 0)
    inside = (slot >= low_slot) & (slot < low_slot + capacity)
    spread = jnp.where(inside, 1.0, 0.0).astype(jnp.bfloat16)
    place = jnp.sum(jnp.where(inside, slot - low_slot, 0), 1, keepdims=True).astype(jnp.float32)
    wide = jnp.concatenate([held, high, low], 1).astype(jnp.bfloat16)
    wide = dot32(spread, wide)
    taken = wide[:, 0:tokens] == place
    factors = [
        jnp.where(taken, wide[:, k * tokens : (k + 1) * tokens], 0.0).astype(jnp.bfloat16)
        for k in (1, 2)
    ]
    return jnp.where(taken, 1.0, 0.0).astype(jnp.bfloat16), factors


def mixer_kernel(
    where_ref, routes_ref, weights_ref, docs_ref, gs_ref, stream_ref, gain_ref, gw_ref, ow_ref,
    *refs
):
    resid_ref, upper_ref, lower_ref, ext_ref = refs[-4:]
    parts = ext_ref.shape[0]
    groups, width, _ = gw_ref.shape
    tokens = stream_ref.shape[0]
    mixed = pool_rows(where_ref, docs_ref, refs[:parts], refs[parts : 2 * parts], ext_ref, groups)
    scaled = []
    for g in range(groups):
        lanes = slice(g * width, (g + 1) * width)
        scaled.append((dot32(mixed[g], gw_ref[g]) * gs_ref[:, lanes]).astype(jnp.bfloat16))
    mixer_out = dot32(jnp.concatenate(scaled, 1), ow_ref[...])
    resid = (stream_ref[...].astype(jnp.float32) + mixer_out).astype(jnp.bfloat16)
    resid_ref[...] = resid
    values = resid.astype(jnp.float32)
    inverse = lax.rsqrt(jnp.mean(values * values, -1, keepdims=True) + norm_eps)
    normed = (values * inverse * gain_ref[...]).astype(jnp.bfloat16)
    half = upper_ref.shape[0]
    upper_ref[...] = normed[0:half]
    lower_ref[0 : tokens - half, :] = normed[half:]
    top = routes_ref.shape[0]
    weights = weights_ref[...]
    high = weights.astype(jnp.bfloat16)
    low = (weights - high.astype(jnp.float32)).astype(jnp.bfloat16)
    routes_t = routes_ref[...]
    lines = [piece.astype(jnp.float32)[j : j + 1, :] for piece in (routes_t, high, low)
             for j in range(top)]
    line = jnp.concatenate(lines, 1)
    line = jnp.pad(line, ((0, 0), (0, lower_ref.shape[1] - line.shape[1])))
    rest = lower_ref.shape[0] - (tokens - half)
    lower_ref[tokens - half :, :] = jnp.broadcast_to(line, (rest, line.shape[1])).astype(jnp.bfloat16)


def read_table(lower_ref, tokens, top):
    line = lower_ref[lower_ref.shape[0] - 8 :, :].astype(jnp.float32)
    rows = [line[0:1, j * tokens : (j + 1) * tokens] for j in range(3 * top)]
    pieces = [jnp.concatenate(rows[k * top : (k + 1) * top], 0) for k in range(3)]
    return pieces[0].astype(jnp.int32), pieces[1], pieces[2]


def call(kernel, shapes, args, flops, scratch=(), limit=VMEM_BYTES):
    specs = [pl.BlockSpec(memory_space=pltpu.SMEM)]
    specs += [pl.BlockSpec(memory_space=pltpu.VMEM)] * (len(args) - 1)
    return pl.pallas_call(
        kernel,
        out_shape=tuple(shapes),
        in_specs=specs,
        out_specs=(pl.BlockSpec(memory_space=pltpu.VMEM),) * len(shapes),
        scratch_shapes=scratch,
        compiler_params=pltpu.CompilerParams(vmem_limit_bytes=limit),
        cost_estimate=pl.CostEstimate(
            flops=flops, transcendentals=0, bytes_accessed=sum(a.nbytes for a in args)
        ),
    )(*args)


def pick_kernel(where_ref, *refs, tokens, top, capacity):
    chunk_refs, send_refs, factor_ref = refs[: 2 * CORES], refs[2 * CORES : -1], refs[-1]
    chips = len(send_refs)
    tables = [read_table(chunk_refs[2 * k + 1], tokens, top) for k in range(CORES)]
    taken, factors = slot_tables(where_ref, tables, chips, capacity)
    size = chips * capacity
    for k in range(CORES):
        upper_ref, lower_ref = chunk_refs[2 * k : 2 * k + 2]
        rest = tokens - upper_ref.shape[0]
        rows = jnp.concatenate([upper_ref[...], lower_ref[0:rest, :]], 0)
        part = slice(k * size, (k + 1) * size)
        picked = dot32(taken[part], rows).astype(jnp.bfloat16)
        for d in range(chips):
            rows = picked[d * capacity : (d + 1) * capacity]
            send_refs[d][k * capacity : (k + 1) * capacity, :] = rows
        for f in range(2):
            start = (2 * k + f) * size
            factor_ref[start : start + size, :] = factors[f][part]


def weighted_sum(factor_ref, back_refs, k, capacity):
    size = 2 * len(back_refs) * capacity
    back = [ref[k * capacity : (k + 1) * capacity, :] for ref in back_refs]
    return lax.dot_general(
        factor_ref[k * size : (k + 1) * size, :], jnp.concatenate(back + back, 0),
        (((0,), (0,)), ((), ())), preferred_element_type=jnp.float32,
    )


def share_kernel(where_ref, factor_ref, *refs, capacity):
    back_refs, (given_ref, kept_ref) = refs[:-2], refs[-2:]
    given_ref[...] = weighted_sum(factor_ref, back_refs, 1, capacity).astype(jnp.bfloat16)
    kept_ref[...] = weighted_sum(factor_ref, back_refs, 0, capacity)


def sum_kernel(where_ref, kept_ref, got_ref, *refs, start):
    size = refs[-1].shape[0]
    rows = slice(start, start + size)
    total = kept_ref[rows, :] + got_ref[rows, :].astype(jnp.float32)
    for ref in refs[:-1]:
        total = total + ref[...].astype(jnp.float32)
    refs[-1][...] = total.astype(jnp.bfloat16)


def final_kernel(where_ref, kept_ref, got_ref, resid_ref, *refs):
    total = kept_ref[...] + got_ref[...].astype(jnp.float32) + resid_ref[...].astype(jnp.float32)
    if len(refs) > 1:
        total = total + jnp.concatenate([ref[...] for ref in refs[:-1]], 0).astype(jnp.float32)
    refs[-1][...] = total.astype(jnp.bfloat16)


def expert_kernel(where_ref, *refs):
    chips = (len(refs) - 3) // 2
    row_refs, (gate_ref, up_ref, down_ref), out_refs = refs[:chips], refs[chips : chips + 3], refs[chips + 3 :]
    rows = jnp.concatenate([ref[...] for ref in row_refs], 0)
    hidden = gate_ref.shape[1]
    cut = min(hidden, 256)
    total = None
    for start in range(0, hidden, cut):
        lanes = slice(start, start + cut)
        gated = jnp.minimum(dot32(rows, gate_ref[:, lanes]), clamp_limit)
        linear = jnp.clip(dot32(rows, up_ref[:, lanes]), -clamp_limit, clamp_limit)
        activated = (gated * jax.nn.sigmoid(sigmoid_alpha * gated) * (linear + 1.0)).astype(
            jnp.bfloat16
        )
        part = dot32(activated, down_ref[lanes, :])
        total = part if total is None else total + part
    result = total.astype(jnp.bfloat16)
    length = row_refs[0].shape[0]
    for d in range(chips):
        out_refs[d][...] = result[d * length : (d + 1) * length]


in_vmem = functools.partial(pltpu.with_memory_space_constraint, memory_space=pltpu.VMEM)


def body(
    stream,
    projected,
    segments,
    group_weight,
    group_scale,
    out_weight,
    ffn_gain,
    routes,
    route_weights,
    expert_gate,
    expert_up,
    expert_down,
    *,
    planes,
):
    row_count, channels = projected.shape
    tp_count = lax.axis_size("tp")
    sp_count = lax.axis_size("sp")
    width = channels * tp_count
    group_width = width // GROUPS
    tokens, top = routes.shape
    devices = sp_count * tp_count
    count = devices // planes
    chips = count // CORES
    capacity = 3 * tokens * top // (2 * devices)
    hidden = expert_gate.shape[2]
    every = ("sp", "tp")
    sp_index, tp_index = lax.axis_index("sp"), lax.axis_index("tp")
    device = sp_index * tp_count + tp_index
    where = jnp.stack(
        [device // count, tp_index, device % count // CORES, device % CORES, sp_index]
    ).astype(jnp.int32)
    sizes = dict(tokens=tokens, top=top, capacity=capacity)

    def move(value, to):
        return lax.ppermute(value, every, [(i, to(i)) for i in range(devices)])

    ring = list(range(1, planes, 2)) + list(range((planes - 1) // 2 * 2, -1, -2))
    after = {ring[k - 1]: plane for k, plane in enumerate(ring)}

    def hop(value):
        return move(value, lambda i: after[i // count] * count + i % count)

    def swap(value):
        return move(value, lambda i: i ^ 1)

    def in_plane(blocks):
        moved = [blocks[0]]
        for d in range(1, chips):
            moved.append(move(blocks[d], lambda i: i ^ (d * CORES)))
        return moved

    rim = longest_window
    docs = segments.reshape(tp_count, tokens)
    part = jax.ShapeDtypeStruct((tokens + rim, channels), jnp.bfloat16)
    *cuts, tail = call(
        cut_kernel,
        [part] * tp_count + [jax.ShapeDtypeStruct((rim, channels), jnp.bfloat16)],
        [where, projected, docs],
        COVER_FLOPS,
        [pltpu.VMEM((row_count + rim, channels), jnp.bfloat16)],
    )

    rims = [move(tail, lambda i: (i + tp_count) % devices)]
    blocks = [cuts[0]]
    for d in range(1, tp_count):
        blocks.append(move(cuts[d], lambda i: i ^ d))
    for d in range(1, tp_count):
        rims.append(move(rims[0], lambda i: i ^ d))

    shape = jax.ShapeDtypeStruct((tokens, width), jnp.bfloat16)
    block = jax.ShapeDtypeStruct((CORES * capacity, width), jnp.bfloat16)
    half = tokens // 2
    piece = jax.ShapeDtypeStruct((half, width), jnp.bfloat16)
    resid, *chunk = call(
        mixer_kernel,
        [shape, piece, jax.ShapeDtypeStruct((tokens - half + 8, width), jnp.bfloat16)],
        [
            where, routes.T, route_weights.T, docs, in_vmem(group_scale.reshape(1, -1)),
            in_vmem(stream), in_vmem(ffn_gain.reshape(1, -1)), in_vmem(group_weight),
            in_vmem(out_weight), *blocks, *rims,
        ],
        2 * tokens * width * (width + group_width),
        [pltpu.VMEM((tp_count, tokens + rim, channels), jnp.bfloat16)],
    )
    small = 2 * tokens * count * capacity * width
    matrices = [in_vmem(expert_gate[0]), in_vmem(expert_up[0]), in_vmem(expert_down[0])]

    factor = jax.ShapeDtypeStruct((2 * count * capacity, tokens), jnp.bfloat16)

    def dispatch(pair):
        *rows, factors = call(
            functools.partial(pick_kernel, **sizes), [block] * chips + [factor],
            [where, *pair], small,
        )
        return in_plane(rows), factors

    def experts(rows):
        results = call(
            expert_kernel, [block] * chips, [where, *rows, *matrices],
            6 * count * capacity * width * hidden,
        )
        return in_plane(results)

    def share(factors, back):
        given, kept = call(
            functools.partial(share_kernel, capacity=capacity),
            [shape, jax.ShapeDtypeStruct(shape.shape, jnp.float32)],
            [where, factors, *back], 2 * small,
        )
        return kept, swap(given)

    chunks = [chunk]
    for _ in range(1, planes):
        chunks.append([hop(chunks[-1][h]) for h in range(2)])
    pairs = []
    for s in range(planes):
        pairs.append(chunks[s] + [swap(chunks[s][h]) for h in range(2)])
    arrived = [dispatch(pairs[s]) for s in range(planes)]
    returned = [experts(arrived[s][0]) for s in range(planes)]
    carried = [[], []]
    for s in range(1, planes):
        shares = share(arrived[s][1], returned[s])
        for h in range(2):
            (total,) = call(
                functools.partial(sum_kernel, start=h * half), [piece],
                [where, *shares, *carried[h]], tokens * width,
            )
            carried[h] = [hop(total)]
    shares = share(arrived[0][1], returned[0])
    (out,) = call(
        final_kernel, [shape], [where, *shares, resid, *carried[0], *carried[1]],
        tokens * width,
    )
    return out


def plane_count(mesh):
    sizes = mesh.shape
    heights = {getattr(d, "coords", (0, 0, -1))[2] for d in mesh.devices.flat}
    if -1 in heights:
        return max(1, sizes["sp"] // max(1, sizes["tp"] // 2))
    return len(heights)


def solution(mesh):
    in_specs = (
        P(("sp", "tp"), None),
        P("sp", "tp"),
        P("sp"),
        P(),
        P(),
        P(),
        P(),
        P(("sp", "tp"), None),
        P(("sp", "tp"), None),
        P(("sp", "tp"), None, None),
        P(("sp", "tp"), None, None),
        P(("sp", "tp"), None, None),
    )
    out_specs = P(("sp", "tp"), None)
    planes = plane_count(mesh)

    def layer(*args):
        return body(*args, planes=planes)

    return jax.shard_map(layer, mesh=mesh, in_specs=in_specs, out_specs=out_specs, check_vma=False)
```

```python
import functools

import jax
import jax.numpy as jnp
from jax import lax
from jax.experimental import pallas as pl
from jax.experimental.pallas import tpu as pltpu
from jax.sharding import PartitionSpec as P


GROUPS = 4
CORES = 2
HIDDEN_CUT = 256
DOWN_CUT = 2048
COVER_FLOPS = 40_000_000_000

norm_eps = 1e-05
clamp_limit = 7.0
sigmoid_alpha = 1.702
longest_window = 16
VMEM_BYTES = 12 * 1024 * 1024


def dot32(a, b):
    return jnp.dot(a, b, preferred_element_type=jnp.float32)


def cut_kernel(where_ref, rows_ref, docs_ref, *refs):
    out_refs, rim_ref, ext_ref = refs[:-2], refs[-2], refs[-1]
    row_count, channels = rows_ref.shape
    rim = rim_ref.shape[0]
    block = row_count // len(out_refs)
    ext_ref[0:rim, :] = jnp.zeros((rim, channels), jnp.bfloat16)
    ext_ref[rim:, :] = rows_ref[...]
    for d in range(len(out_refs)):
        start = pl.multiple_of((where_ref[1] ^ d) * block, block)
        out_refs[d][...] = ext_ref[pl.ds(start, block + rim), :]
    docs = docs_ref[docs_ref.shape[0] - 1 :, :][:, block - rim :] + 1
    line = jnp.concatenate(
        [docs.astype(jnp.float32), jnp.zeros((1, channels - rim), jnp.float32)], 1
    )
    tail = rows_ref[row_count - rim :, :].astype(jnp.float32)
    first = lax.broadcasted_iota(jnp.int32, (rim, channels), 0) == 0
    rim_ref[...] = jnp.where(first, line, tail).astype(jnp.bfloat16)


def pool_rows(where_ref, docs_ref, block_refs, rim_refs, ext_ref, groups):
    mine = where_ref[1]
    parts, tokens_rim, channels = ext_ref.shape
    rim = rim_refs[0].shape[0]
    block = tokens_rim - rim
    for d in range(parts):
        ext_ref[mine ^ d] = block_refs[d][...]

    @pl.when(mine == 0)
    def _():
        for d in range(parts):
            ext_ref[d, 0:rim, :] = rim_refs[d][...]

    rim_docs = (rim_refs[0][0:1, 0:rim].astype(jnp.float32) - 1.0).astype(jnp.int32)
    rim_docs = jnp.where(where_ref[4] == 0, -1, rim_docs)
    here = docs_ref[pl.ds(mine, 1), :]
    previous = docs_ref[pl.ds(jnp.maximum(mine - 1, 0), 1), :][:, block - rim :]
    col_docs = jnp.concatenate([jnp.where(mine == 0, rim_docs, previous), here], 1)
    at_row = lax.broadcasted_iota(jnp.int32, (block, tokens_rim), 0)
    at_col = lax.broadcasted_iota(jnp.int32, (block, tokens_rim), 1)
    back = at_row + rim - at_col
    row_docs = jnp.sum(
        jnp.where(back == 0, jnp.broadcast_to(col_docs, back.shape), 0), 1, keepdims=True
    )
    alike = (col_docs == row_docs) & (back >= 0)
    values = jnp.concatenate([ext_ref[d] for d in range(parts)], 1)
    width = parts * channels // groups
    mixed = []
    for g in range(groups):
        lanes = values[:, g * width : (g + 1) * width]
        band = jnp.where(alike & (back < 2 << g), 1.0, 0.0)
        count = jnp.sum(band, 1, keepdims=True)
        total = dot32(band.astype(jnp.bfloat16), lanes)
        mixed.append((total / count - lanes[rim:, :].astype(jnp.float32)).astype(jnp.bfloat16))
    return mixed


def slot_tables(where_ref, tables, chips, capacity):
    tokens = tables[0][0].shape[1]
    offset = lax.broadcasted_iota(jnp.int32, (chips, tokens), 0)
    here = (offset ^ where_ref[2]) * CORES + where_ref[3] + where_ref[0] * (chips * CORES)
    named, highs, lows = [], [], []
    for routes_t, high, low in tables:
        matches = [routes_t[j : j + 1, :] == here for j in range(routes_t.shape[0])]
        named.append(sum(jnp.where(m, 1.0, 0.0) for m in matches))
        highs.append(sum(jnp.where(m, high[j : j + 1, :], 0.0) for j, m in enumerate(matches)))
        lows.append(sum(jnp.where(m, low[j : j + 1, :], 0.0) for j, m in enumerate(matches)))
    named, high, low = (jnp.concatenate(parts, 0) for parts in (named, highs, lows))
    lines = named.shape[0]
    earlier = (
        lax.broadcasted_iota(jnp.int32, (tokens, tokens), 0)
        < lax.broadcasted_iota(jnp.int32, (tokens, tokens), 1)
    )
    rank = dot32(named.astype(jnp.bfloat16), jnp.where(earlier, 1.0, 0.0).astype(jnp.bfloat16))
    held = jnp.where(named > 0.0, rank, -1.0)
    slots = lines * capacity
    low_slot = lax.broadcasted_iota(jnp.int32, (slots, lines), 1) * capacity
    slot = lax.broadcasted_iota(jnp.int32, (slots, lines), 0)
    inside = (slot >= low_slot) & (slot < low_slot + capacity)
    spread = jnp.where(inside, 1.0, 0.0).astype(jnp.bfloat16)
    place = jnp.sum(jnp.where(inside, slot - low_slot, 0), 1, keepdims=True).astype(jnp.float32)
    wide = jnp.concatenate([held, high, low], 1).astype(jnp.bfloat16)
    wide = dot32(spread, wide)
    taken = wide[:, 0:tokens] == place
    factors = [
        jnp.where(taken, wide[:, k * tokens : (k + 1) * tokens], 0.0).astype(jnp.bfloat16)
        for k in (1, 2)
    ]
    return jnp.where(taken, 1.0, 0.0).astype(jnp.bfloat16), factors


def mixer_kernel(
    where_ref, routes_ref, weights_ref, docs_ref, gs_ref, stream_ref, gain_ref, gw_ref, ow_ref,
    *refs
):
    resid_ref, upper_ref, lower_ref, ext_ref = refs[-4:]
    parts = ext_ref.shape[0]
    groups, width, _ = gw_ref.shape
    tokens = stream_ref.shape[0]
    mixed = pool_rows(where_ref, docs_ref, refs[:parts], refs[parts : 2 * parts], ext_ref, groups)
    scaled = []
    for g in range(groups):
        lanes = slice(g * width, (g + 1) * width)
        scaled.append((dot32(mixed[g], gw_ref[g]) * gs_ref[:, lanes]).astype(jnp.bfloat16))
    mixer_out = dot32(jnp.concatenate(scaled, 1), ow_ref[...])
    resid = (stream_ref[...].astype(jnp.float32) + mixer_out).astype(jnp.bfloat16)
    resid_ref[...] = resid
    values = resid.astype(jnp.float32)
    inverse = lax.rsqrt(jnp.mean(values * values, -1, keepdims=True) + norm_eps)
    normed = (values * inverse * gain_ref[...]).astype(jnp.bfloat16)
    half = upper_ref.shape[0]
    upper_ref[...] = normed[0:half]
    lower_ref[0 : tokens - half, :] = normed[half:]
    top = routes_ref.shape[0]
    weights = weights_ref[...]
    high = weights.astype(jnp.bfloat16)
    low = (weights - high.astype(jnp.float32)).astype(jnp.bfloat16)
    routes_t = routes_ref[...]
    lines = [piece.astype(jnp.float32)[j : j + 1, :] for piece in (routes_t, high, low)
             for j in range(top)]
    line = jnp.concatenate(lines, 1)
    line = jnp.pad(line, ((0, 0), (0, lower_ref.shape[1] - line.shape[1])))
    rest = lower_ref.shape[0] - (tokens - half)
    lower_ref[tokens - half :, :] = jnp.broadcast_to(line, (rest, line.shape[1])).astype(jnp.bfloat16)


def read_table(lower_ref, tokens, top):
    line = lower_ref[lower_ref.shape[0] - 8 :, :].astype(jnp.float32)
    rows = [line[0:1, j * tokens : (j + 1) * tokens] for j in range(3 * top)]
    pieces = [jnp.concatenate(rows[k * top : (k + 1) * top], 0) for k in range(3)]
    return pieces[0].astype(jnp.int32), pieces[1], pieces[2]


def call(kernel, shapes, args, flops, scratch=(), limit=VMEM_BYTES):
    specs = [pl.BlockSpec(memory_space=pltpu.SMEM)]
    specs += [pl.BlockSpec(memory_space=pltpu.VMEM)] * (len(args) - 1)
    return pl.pallas_call(
        kernel,
        out_shape=tuple(shapes),
        in_specs=specs,
        out_specs=(pl.BlockSpec(memory_space=pltpu.VMEM),) * len(shapes),
        scratch_shapes=scratch,
        compiler_params=pltpu.CompilerParams(vmem_limit_bytes=limit),
        cost_estimate=pl.CostEstimate(
            flops=flops, transcendentals=0, bytes_accessed=sum(a.nbytes for a in args)
        ),
    )(*args)


def pick_kernel(where_ref, *refs, tokens, top, capacity):
    chunk_refs, send_refs, factor_ref = refs[: 2 * CORES], refs[2 * CORES : -1], refs[-1]
    chips = len(send_refs)
    tables = [read_table(chunk_refs[2 * k + 1], tokens, top) for k in range(CORES)]
    taken, factors = slot_tables(where_ref, tables, chips, capacity)
    size = chips * capacity
    for k in range(CORES):
        upper_ref, lower_ref = chunk_refs[2 * k : 2 * k + 2]
        rest = tokens - upper_ref.shape[0]
        rows = jnp.concatenate([upper_ref[...], lower_ref[0:rest, :]], 0)
        part = slice(k * size, (k + 1) * size)
        picked = dot32(taken[part], rows).astype(jnp.bfloat16)
        for d in range(chips):
            rows = picked[d * capacity : (d + 1) * capacity]
            send_refs[d][k * capacity : (k + 1) * capacity, :] = rows
        for f in range(2):
            start = (2 * k + f) * size
            factor_ref[start : start + size, :] = factors[f][part]


def weighted_sum(factor_ref, back_refs, k, capacity):
    size = 2 * len(back_refs) * capacity
    back = [ref[k * capacity : (k + 1) * capacity, :] for ref in back_refs]
    return lax.dot_general(
        factor_ref[k * size : (k + 1) * size, :], jnp.concatenate(back + back, 0),
        (((0,), (0,)), ((), ())), preferred_element_type=jnp.float32,
    )


def share_kernel(where_ref, factor_ref, *refs, capacity):
    back_refs, given_refs, kept_ref = refs[:-3], refs[-3:-1], refs[-1]
    given = weighted_sum(factor_ref, back_refs, 1, capacity).astype(jnp.bfloat16)
    half = given_refs[0].shape[0]
    given_refs[0][...] = given[:half]
    given_refs[1][...] = given[half:]
    kept_ref[...] = weighted_sum(factor_ref, back_refs, 0, capacity)


def sum_kernel(where_ref, kept_ref, got_ref, *refs, start):
    size = refs[-1].shape[0]
    rows = slice(start, start + size)
    total = kept_ref[rows, :] + got_ref[...].astype(jnp.float32)
    for ref in refs[:-1]:
        total = total + ref[...].astype(jnp.float32)
    refs[-1][...] = total.astype(jnp.bfloat16)


def final_kernel(where_ref, kept_ref, resid_ref, *refs, count):
    total = kept_ref[...] + resid_ref[...].astype(jnp.float32)
    for ref in refs[:count]:
        total = total + ref[...].astype(jnp.float32)
    refs[-1][...] = total.astype(jnp.bfloat16)


def final_half(where, h, kept, resid, pieces, so_far):
    size, width = pieces[0].shape
    part = pl.BlockSpec((size, width), lambda i: (h, 0))
    whole = pl.BlockSpec((size, width), lambda i: (0, 0))
    args = [where, kept, resid, *pieces] + ([] if so_far is None else [so_far])
    rest = [] if so_far is None else [pl.BlockSpec(memory_space=pl.ANY)]
    return pl.pallas_call(
        functools.partial(final_kernel, count=len(pieces)),
        grid=(1,),
        out_shape=jax.ShapeDtypeStruct(resid.shape, jnp.bfloat16),
        in_specs=[pl.BlockSpec(memory_space=pltpu.SMEM), part, part] + [whole] * len(pieces) + rest,
        out_specs=part,
        input_output_aliases={} if so_far is None else {len(args) - 1: 0},
        compiler_params=pltpu.CompilerParams(vmem_limit_bytes=VMEM_BYTES),
        cost_estimate=pl.CostEstimate(
            flops=resid.size, transcendentals=0, bytes_accessed=4 * resid.size
        ),
        name="final",
    )(*args)


def expert_kernel(where_ref, *refs):
    chips = (len(refs) - 3) // 2
    row_refs, matrices, out_refs = refs[:chips], refs[chips : chips + 3], refs[chips + 3 :]
    gate_ref, up_ref, down_ref = matrices
    rows = jnp.concatenate([ref[...] for ref in row_refs], 0)
    hidden = gate_ref.shape[1]
    cut = min(hidden, HIDDEN_CUT)
    parts = []
    for start in range(0, hidden, cut):
        lanes = slice(start, start + cut)
        gated = jnp.minimum(dot32(rows, gate_ref[:, lanes]), clamp_limit)
        linear = jnp.clip(dot32(rows, up_ref[:, lanes]), -clamp_limit, clamp_limit)
        activated = gated * jax.nn.sigmoid(sigmoid_alpha * gated) * (linear + 1.0)
        parts.append(activated.astype(jnp.bfloat16))
    activated = jnp.concatenate(parts, 1)
    width = down_ref.shape[1]
    cut = min(width, DOWN_CUT)
    result = jnp.concatenate(
        [
            dot32(activated, down_ref[:, start : start + cut]).astype(jnp.bfloat16)
            for start in range(0, width, cut)
        ],
        1,
    )
    length = row_refs[0].shape[0]
    for d in range(chips):
        out_refs[d][...] = result[d * length : (d + 1) * length]


in_vmem = functools.partial(pltpu.with_memory_space_constraint, memory_space=pltpu.VMEM)


def body(
    stream,
    projected,
    segments,
    group_weight,
    group_scale,
    out_weight,
    ffn_gain,
    routes,
    route_weights,
    expert_gate,
    expert_up,
    expert_down,
    *,
    planes,
):
    row_count, channels = projected.shape
    tp_count = lax.axis_size("tp")
    sp_count = lax.axis_size("sp")
    width = channels * tp_count
    group_width = width // GROUPS
    tokens, top = routes.shape
    devices = sp_count * tp_count
    count = devices // planes
    chips = count // CORES
    capacity = 3 * tokens * top // (2 * devices)
    hidden = expert_gate.shape[2]
    every = ("sp", "tp")
    sp_index, tp_index = lax.axis_index("sp"), lax.axis_index("tp")
    device = sp_index * tp_count + tp_index
    where = jnp.stack(
        [device // count, tp_index, device % count // CORES, device % CORES, sp_index]
    ).astype(jnp.int32)
    sizes = dict(tokens=tokens, top=top, capacity=capacity)

    def move(value, to):
        return lax.ppermute(value, every, [(i, to(i)) for i in range(devices)])

    ring = list(range(1, planes, 2)) + list(range((planes - 1) // 2 * 2, -1, -2))
    after = {ring[k - 1]: plane for k, plane in enumerate(ring)}

    def hop(value):
        return move(value, lambda i: after[i // count] * count + i % count)

    def swap(value):
        return move(value, lambda i: i ^ 1)

    def in_plane(blocks):
        moved = [blocks[0]]
        for d in range(1, chips):
            moved.append(move(blocks[d], lambda i: i ^ (d * CORES)))
        return moved

    rim = longest_window
    docs = segments.reshape(tp_count, tokens)
    part = jax.ShapeDtypeStruct((tokens + rim, channels), jnp.bfloat16)
    *cuts, tail = call(
        cut_kernel,
        [part] * tp_count + [jax.ShapeDtypeStruct((rim, channels), jnp.bfloat16)],
        [where, projected, docs],
        COVER_FLOPS,
        [pltpu.VMEM((row_count + rim, channels), jnp.bfloat16)],
    )

    rims = [move(tail, lambda i: (i + tp_count) % devices)]
    blocks = [cuts[0]]
    for d in range(1, tp_count):
        blocks.append(move(cuts[d], lambda i: i ^ d))
    for d in range(1, tp_count):
        rims.append(move(rims[0], lambda i: i ^ d))

    shape = jax.ShapeDtypeStruct((tokens, width), jnp.bfloat16)
    block = jax.ShapeDtypeStruct((CORES * capacity, width), jnp.bfloat16)
    half = tokens // 2
    piece = jax.ShapeDtypeStruct((half, width), jnp.bfloat16)
    resid, *chunk = call(
        mixer_kernel,
        [shape, piece, jax.ShapeDtypeStruct((tokens - half + 8, width), jnp.bfloat16)],
        [
            where, routes.T, route_weights.T, docs, in_vmem(group_scale.reshape(1, -1)),
            in_vmem(stream), in_vmem(ffn_gain.reshape(1, -1)), in_vmem(group_weight),
            in_vmem(out_weight), *blocks, *rims,
        ],
        2 * tokens * width * (width + group_width),
        [pltpu.VMEM((tp_count, tokens + rim, channels), jnp.bfloat16)],
    )
    small = 2 * tokens * count * capacity * width
    matrices = [in_vmem(expert_gate[0]), in_vmem(expert_up[0]), in_vmem(expert_down[0])]

    factor = jax.ShapeDtypeStruct((2 * count * capacity, tokens), jnp.bfloat16)

    def dispatch(pair):
        *rows, factors = call(
            functools.partial(pick_kernel, **sizes), [block] * chips + [factor],
            [where, *pair], small,
        )
        return in_plane(rows), factors

    def experts(rows):
        results = call(
            expert_kernel, [block] * chips, [where, *rows, *matrices],
            6 * count * capacity * width * hidden,
        )
        return in_plane(results)

    def share(factors, back):
        *given, kept = call(
            functools.partial(share_kernel, capacity=capacity),
            [piece, piece, jax.ShapeDtypeStruct(shape.shape, jnp.float32)],
            [where, factors, *back], 2 * small,
        )
        return kept, [swap(given[h]) for h in range(2)]

    chunks = [chunk]
    for _ in range(1, planes):
        chunks.append([hop(chunks[-1][h]) for h in range(2)])
    pairs = []
    for s in range(planes):
        pairs.append(chunks[s] + [swap(chunks[s][h]) for h in range(2)])
    arrived = [dispatch(pairs[s]) for s in range(planes)]
    returned = [experts(arrived[s][0]) for s in range(planes)]
    carried = [[], []]
    for s in range(1, planes):
        kept, got = share(arrived[s][1], returned[s])
        for h in range(2):
            (total,) = call(
                functools.partial(sum_kernel, start=h * half), [piece],
                [where, kept, got[h], *carried[h]], tokens * width,
            )
            carried[h] = [hop(total)]
    kept, got = share(arrived[0][1], returned[0])
    out = None
    for h in range(2):
        out = final_half(where, h, kept, resid, [got[h], *carried[h]], out)
    return out


def plane_count(mesh):
    sizes = mesh.shape
    heights = {getattr(d, "coords", (0, 0, -1))[2] for d in mesh.devices.flat}
    if -1 in heights:
        return max(1, sizes["sp"] // max(1, sizes["tp"] // 2))
    return len(heights)


def solution(mesh):
    in_specs = (
        P(("sp", "tp"), None),
        P("sp", "tp"),
        P("sp"),
        P(),
        P(),
        P(),
        P(),
        P(("sp", "tp"), None),
        P(("sp", "tp"), None),
        P(("sp", "tp"), None, None),
        P(("sp", "tp"), None, None),
        P(("sp", "tp"), None, None),
    )
    out_specs = P(("sp", "tp"), None)
    planes = plane_count(mesh)

    def layer(*args):
        return body(*args, planes=planes)

    return jax.shard_map(layer, mesh=mesh, in_specs=in_specs, out_specs=out_specs, check_vma=False)
```
